512 devices in a mesh: ep: 32 (over z, core), tp: 16 (over y, x).
Axes of the slice: x: 4, y: 4, z: 16, core: 2. Of those that a mesh axis runs over, the one named last changes fastest.
Arguments:
- query_rows: bfloat16 [24576, 1024], P('ep', 'tp'), may hold values from -600 to 600
- key_rows: bfloat16 [24576, 1024], P('ep', 'tp'), may hold values from -6 to 6
- value_rows: bfloat16 [24576, 1024], P('ep', 'tp'), may hold values from -6 to 6
- cum_gate: float32 [16, 24576], P('tp'), may hold values from -2458 to 0, as said below
- out_weight: bfloat16 [1024, 2048], P(None, 'tp'), may hold values from -0.1875 to 0.1875
- moe_input: bfloat16 [6144, 2048], P('ep'), may hold values from -6 to 6
- moe_gain: float32 [2048], replicated, may hold values from 0.1 to 1.9
- routes: int32 [6144, 3], P('ep'), may hold values from 0 to 127, all different within a row; in each aligned block of 192 rows (0 to 191, 192 to 383, ...) at most 9 rows name the same one
- route_weight: float32 [6144, 3], P('ep'), may hold values from 0.2 to 1.5
- expert_gate: bfloat16 [128, 2048, 512], P('ep', None, 'tp'), may hold values from -0.125 to 0.125
- expert_up: bfloat16 [128, 2048, 512], P('ep', None, 'tp'), may hold values from -0.125 to 0.125
- expert_down: bfloat16 [128, 512, 2048], P('ep', None, 'tp'), may hold values from -0.25 to 0.25
- shared_gate: bfloat16 [2048, 512], P(None, 'tp'), may hold values from -0.125 to 0.125
- shared_up: bfloat16 [2048, 512], P(None, 'tp'), may hold values from -0.125 to 0.125
- shared_down: bfloat16 [512, 2048], P(None, 'tp'), may hold values from -0.25 to 0.25
Outputs:
- mixer_out: bfloat16 [24576, 2048], P('ep', 'tp')
- moe_out: bfloat16 [6144, 2048], P('ep', 'tp')
The draws below stay inside these ranges and needn't reach their ends.
Inputs may be any that keep to these rules, and one draw needn't show every extreme that they name: Non-increasing along positions: cum_gate[h, t] is the sum of the log forget gates of head h over positions 0 to t. `routes`: the 3 experts of a token differ. In each aligned block of 192 tokens no expert is named by more than 9 tokens, a bound that some block reaches.
All inputs are finite; a program needn't handle non-finite values.
Results may differ from the reference program's by a relative error of at most 0.0068.
Values may be sent and summed in bfloat16 or wider, within the bound.
A program may use at most 64 MiB of HBM per device.

```python
import math
import jax
import jax.numpy as jnp
import numpy as np
from jax import lax

D = 2048
HEADS = 16
HEAD = 64
FF = 512
FS = 512
EXPERTS = 128
TOP = 3
SEQ_DEV = 768
LENGTH = 24576
MOE_DEV = 192
TOKENS_MOE = 6144
CAP = 9
N_EP = 32


def draw_query_rows(key, part):
    base_key = jax.random.fold_in(key, 7)
    key_normal = jax.random.fold_in(base_key, 0)
    drawn = jnp.clip(jax.random.normal(key_normal, (LENGTH, HEADS * HEAD), jnp.float32), -6.0, 6.0)
    return drawn.astype(jnp.bfloat16)


def draw_cum_gate(key, part):
    base_key = jax.random.fold_in(key, 13)
    key_heads, key_steps, key_blocks = jax.random.split(base_key, 3)
    head_order = jax.random.permutation(key_heads, HEADS)
    fast_count = HEADS // 2
    decay_rates = jnp.where(head_order < fast_count, 1.0 / 40.0, 1.0 / LENGTH).astype(jnp.float32)
    low = jnp.log(0.5)
    high = jnp.log(2.0)
    step_factors = jnp.exp(jax.random.uniform(key_steps, (HEADS, LENGTH), jnp.float32, low, high))
    block_factors = jnp.exp(jax.random.uniform(key_blocks, (HEADS, LENGTH // SEQ_DEV), jnp.float32, low, high))
    block_factors = jnp.repeat(block_factors, SEQ_DEV, axis=1)
    log_gates = -decay_rates[:, None] * step_factors * block_factors
    return jnp.cumsum(log_gates, axis=1).astype(jnp.float32)


def levels(rng, shape, cuts, least, high):
    def one(axis_at, shards_of):
        draws = jax.random.uniform(jax.random.fold_in(jax.random.fold_in(rng, 6), axis_at), (shards_of,), jnp.float32, least / len(cuts), high / len(cuts))
        return jnp.repeat(jnp.exp(draws), shape[axis_at] // shards_of).reshape((-1,) + (1,) * (len(shape) - axis_at - 1))

    loudness = one(*cuts[0])
    for cut in cuts[1:]:
        loudness = loudness * one(*cut)
    return loudness


def deal_out(rng, own, number, rows, amount, top, limit, slope):
    order = jax.random.permutation(rng, amount)
    heavy_load, common = load_shares(amount, rows * top, limit, slope, True), load_shares(amount, rows * top, limit, slope, False)
    places = jnp.arange(amount)

    def named(tallies, turn):
        used = int((tallies > 0).sum())
        fixed = max(1, used // 4)
        shifted = fixed + (places - fixed + turn * (used - fixed)) % max(1, amount - fixed)
        return jnp.zeros((amount,), jnp.int32).at[order[jnp.where(places < fixed, places, shifted)]].set(jnp.asarray(tallies, jnp.int32))

    tallies = jnp.where(number % 4 == 0, named(heavy_load, number // 4), named(common, number - number // 4 - 1))
    mixed = jax.random.permutation(jax.random.fold_in(own, 3), amount)
    donor, receiver = mixed[0:amount // 2 * 2:2], mixed[1:amount // 2 * 2:2]
    margin = jnp.minimum(tallies[donor] - 1, limit - tallies[receiver]) // 2
    margin = jnp.where((donor == order[0]) | (receiver == order[0]) | (tallies[receiver] == 0), 0, jnp.maximum(margin, 0))
    shifted = jax.random.randint(jax.random.fold_in(own, 4), (amount // 2,), 0, 1 << 20) % (margin + 1)
    tallies = tallies.at[donor].add(-shifted).at[receiver].add(shifted)
    members = jnp.searchsorted(jnp.cumsum(tallies), jnp.arange(rows * top), side="right").astype(jnp.int32)
    listing = members.reshape(top, rows).T
    listing = listing[jax.random.permutation(jax.random.fold_in(own, 1), rows)]
    turn = jax.random.randint(jax.random.fold_in(own, 2), (rows, 1), 0, top)
    return jnp.take_along_axis(listing, (jnp.arange(top)[None, :] + turn) % top, axis=1)


def load_shares(amount, total, reach, skew, full):
    portions = [(1 << 20) // math.isqrt(standing ** skew) + 1 for standing in range(1, amount + 1)]
    largest = reach if full else min(reach, max(-(-total // amount), total * portions[0] // sum(portions)))
    least = 1 if total - largest >= amount - 1 else 0
    holding, rest = [largest] + [least] * (amount - 1), total - largest - least * (amount - 1)
    while rest > 0:
        free = [i for i in range(1, amount) if holding[i] < largest] or [i for i in range(1, amount) if holding[i] < reach]
        pool, left = sum([portions[i] for i in free]), rest
        for i in free:
            more = min(reach - holding[i], max(1, left * portions[i] // pool), rest)
            holding[i] = holding[i] + more
            rest = rest - more
    return np.array(holding)


def bell_draw(stream_key, shape, deviation, limit, cuts=(), kind=jnp.bfloat16):
    array = jax.random.normal(stream_key, shape, jnp.float32) * deviation
    if len(cuts) > 0:
        array = levels(stream_key, shape, cuts, -0.22, 0.18) * array
    return jnp.clip(array, min=-limit, max=limit).astype(kind)


def setup_inputs(seed: int = 0) -> dict:
    keys = jax.random.split(jax.random.key(seed), 16)
    query_rows = draw_query_rows(jax.random.fold_in(keys[15], 71), 0)
    key_rows = bell_draw(keys[1], (LENGTH, HEADS * HEAD), 1.0, 6.0, ((0, 32), (1, 16)))
    value_rows = bell_draw(keys[2], (LENGTH, HEADS * HEAD), 1.0, 6.0, ((0, 32), (1, 16)))
    cum_gate = draw_cum_gate(jax.random.fold_in(keys[15], 71), 0)
    out_weight = bell_draw(keys[4], (HEADS * HEAD, D), (HEADS * HEAD) ** -0.5, 0.1875, ((1, 16),))
    moe_input = bell_draw(keys[5], (TOKENS_MOE, D), 1.0, 6.0, ((0, 32),))
    moe_gain = jnp.clip(1.0 + 0.18 * jax.random.normal(keys[6], (D,), jnp.float32), 0.1, 1.9)
    routes_keys = jax.random.split(jax.random.fold_in(keys[7], 1), TOKENS_MOE // MOE_DEV)
    routes_turns = jax.random.permutation(jax.random.fold_in(keys[7], 3), TOKENS_MOE // MOE_DEV)
    routes = jax.vmap(lambda own, number: deal_out(jax.random.fold_in(keys[7], 2), own, number, MOE_DEV, EXPERTS, TOP, CAP, 2))(routes_keys, routes_turns).reshape((TOKENS_MOE, TOP))
    route_weight = jnp.clip(jnp.exp(math.log(1.5) - 2.014903 * jax.random.uniform(keys[8], (TOKENS_MOE, TOP), jnp.float32) ** levels(keys[8], (TOKENS_MOE, TOP), ((0, 32),), -0.2, 0.2)), 0.2, 1.5)
    expert_gate = bell_draw(keys[9], (EXPERTS, D, FF), D ** -0.5, 0.125, ((0, 32), (2, 16)))
    expert_up = bell_draw(keys[10], (EXPERTS, D, FF), D ** -0.5, 0.125, ((0, 32), (2, 16)))
    expert_down = bell_draw(keys[11], (EXPERTS, FF, D), FF ** -0.5, 0.25, ((0, 32), (2, 16)))
    shared_gate = bell_draw(keys[12], (D, FS), D ** -0.5, 0.125, ((1, 16),))
    shared_up = bell_draw(keys[13], (D, FS), D ** -0.5, 0.125, ((1, 16),))
    shared_down = bell_draw(keys[14], (FS, D), FS ** -0.5, 0.25, ((1, 16),))
    return {"query_rows": query_rows, "key_rows": key_rows, "value_rows": value_rows, "cum_gate": cum_gate, "out_weight": out_weight, "moe_input": moe_input, "moe_gain": moe_gain, "routes": routes, "route_weight": route_weight, "expert_gate": expert_gate, "expert_up": expert_up, "expert_down": expert_down, "shared_gate": shared_gate, "shared_up": shared_up, "shared_down": shared_down}


neg_fill = -1e+30
norm_eps = 1e-06

def attention_heads(query_rows, key_rows, value_rows, cum_gate):
    query_span = 128 if LENGTH % 128 == 0 else LENGTH
    query_heads = query_rows.reshape(LENGTH, HEADS, HEAD)
    key_heads = key_rows.reshape(LENGTH, HEADS, HEAD).astype(jnp.float32)
    value_heads = value_rows.reshape(LENGTH, HEADS, HEAD).astype(jnp.float32)
    key_pos = jnp.arange(LENGTH, dtype=jnp.int32)
    scale = HEAD ** (-0.5)

    def one_block(block_index):
        start = (block_index * query_span).astype(jnp.int32)
        query_block = lax.dynamic_slice_in_dim(query_heads, start, query_span, 0).astype(jnp.float32)
        query_gate = lax.dynamic_slice_in_dim(cum_gate, start, query_span, 1)
        scores = jnp.einsum('qhd,khd->hqk', query_block, key_heads) * scale
        scores = scores + query_gate[:, :, None] - cum_gate[:, None, :]
        query_pos = start + jnp.arange(query_span, dtype=jnp.int32)
        causal = key_pos[None, :] <= query_pos[:, None]
        scores = jnp.where(causal[None], scores, neg_fill)
        row_max = lax.optimization_barrier(jnp.max(scores, axis=2, keepdims=True))
        expon = jnp.where(causal[None], jnp.exp(scores - row_max), 0.0)
        denom = lax.optimization_barrier(jnp.sum(expon, axis=2))
        probs = lax.optimization_barrier(expon.astype(jnp.bfloat16)).astype(jnp.float32)
        summed = jnp.einsum('hqk,khd->qhd', probs, value_heads)
        result = summed / jnp.transpose(denom)[:, :, None]
        return result.astype(jnp.bfloat16).reshape(query_span, HEADS * HEAD)
    blocks = lax.map(one_block, jnp.arange(LENGTH // query_span, dtype=jnp.int32))
    return blocks.reshape(LENGTH, HEADS * HEAD)

def experts_branch(moe_input, moe_gain, routes, route_weight, expert_gate, expert_up, expert_down, shared_gate, shared_up, shared_down):
    moe_rows = moe_input.astype(jnp.float32)
    normed = (moe_rows * lax.rsqrt(lax.optimization_barrier(jnp.mean(moe_rows * moe_rows, axis=1, keepdims=True)) + norm_eps) * moe_gain).astype(jnp.bfloat16)
    pair_count = TOKENS_MOE * TOP
    flat_routes = routes.reshape(-1).astype(jnp.int32)
    one_hot = (flat_routes[:, None] == jnp.arange(EXPERTS, dtype=jnp.int32)[None, :]).astype(jnp.int32)
    one_hot = one_hot.reshape(N_EP, MOE_DEV * TOP, EXPERTS)
    ranks = lax.optimization_barrier(jnp.sum(jnp.cumsum(one_hot, axis=1) * one_hot, axis=2)).reshape(-1) - 1
    block_id = jnp.arange(pair_count, dtype=jnp.int32) // (MOE_DEV * TOP)
    slot_index = (flat_routes * (N_EP * CAP) + block_id * CAP + ranks).astype(jnp.int32)
    pair_token = jnp.arange(pair_count, dtype=jnp.int32) // TOP
    slot_token = jnp.full((EXPERTS * N_EP * CAP,), TOKENS_MOE, jnp.int32).at[slot_index].set(pair_token)
    padded = jnp.concatenate([normed, jnp.zeros((1, D), jnp.bfloat16)], axis=0)

    def one_expert(pieces):
        token_index, gate_w, up_w, down_w = pieces
        gathered = padded[token_index]
        gate_val = jnp.dot(gathered, gate_w, preferred_element_type=jnp.float32)
        up_val = jnp.dot(gathered, up_w, preferred_element_type=jnp.float32)
        hidden = (jax.nn.silu(gate_val) * up_val).astype(jnp.bfloat16)
        return jnp.dot(hidden, down_w, preferred_element_type=jnp.float32).astype(jnp.bfloat16)
    results = lax.map(one_expert, (slot_token.reshape(EXPERTS, N_EP * CAP), expert_gate, expert_up, expert_down))
    picked = results.reshape(EXPERTS * N_EP * CAP, D)[slot_index].astype(jnp.float32).reshape(TOKENS_MOE, TOP, D)
    routed = lax.optimization_barrier(jnp.sum(picked * route_weight[:, :, None], axis=1))
    shared_hidden = (jax.nn.silu(jnp.dot(normed, shared_gate, preferred_element_type=jnp.float32)) * jnp.dot(normed, shared_up, preferred_element_type=jnp.float32)).astype(jnp.bfloat16)
    total = routed + jnp.dot(shared_hidden, shared_down, preferred_element_type=jnp.float32)
    return total.astype(jnp.bfloat16)

def reference(query_rows, key_rows, value_rows, cum_gate, out_weight, moe_input, moe_gain, routes, route_weight, expert_gate, expert_up, expert_down, shared_gate, shared_up, shared_down):
    heads_out = attention_heads(query_rows, key_rows, value_rows, cum_gate)
    mixer_out = jnp.dot(heads_out, out_weight, preferred_element_type=jnp.float32).astype(jnp.bfloat16)
    moe_out = experts_branch(moe_input, moe_gain, routes, route_weight, expert_gate, expert_up, expert_down, shared_gate, shared_up, shared_down)
    return (mixer_out, moe_out)
```

```python
import functools

import jax
import jax.numpy as jnp
import numpy as np
from jax import lax
from jax.experimental import pallas as pl
from jax.experimental.pallas import tpu as pltpu
from jax.sharding import PartitionSpec as P

HEAD = 64
LANES = 128
CORES = 2
TERMS = 4
LOG2E = 1.4426950408889634

neg_fill = -1e30
norm_eps = 1e-06

GATHER_AT = 10
PARTS_AT = 16
HIDDEN_AT = 20
DOWN_AT = 26


def plane_shape(tp_count):
    wide = 1
    while wide * wide < tp_count:
        wide *= 2
    return wide, tp_count // wide


def dot(a, b):
    return jnp.dot(a, b, preferred_element_type=jnp.float32)


def dot_nt(a, b):
    return lax.dot_general(a, b, (((1,), (1,)), ((), ())), preferred_element_type=jnp.float32)


def silu(v):
    return v / (1.0 + jnp.exp(-v))


def loop(count, body, first=0):
    def step(index, carry):
        body(index)
        return carry

    lax.fori_loop(first, count, step, 0)


def layer_kernel(
    cap,
    room,
    q_ref,
    kv_ref,
    terms_ref,
    normed_ref,
    ranks_ref,
    weight_ref,
    places_ref,
    owner_ref,
    gate_w,
    up_w,
    down_ref,
    shared_gate_ref,
    shared_up_ref,
    shared_down_ref,
    out_weight_ref,
    mixer_ref,
    moe_ref,
    held,
    acc,
    row_max,
    picked,
    pieces,
    weights,
    part_out,
    part_in,
    hidden_out,
    hidden_all,
    result_out,
    result_in,
    spread,
    heads_out,
    heads_all,
    up_send,
    down_send,
    side_send,
    kv_recv,
    pick_send,
    pick_recv,
    result_send,
    result_recv,
    piece_send,
    piece_recv,
    weight_send,
    weight_recv,
    part_send,
    part_recv,
    hidden_send,
    hidden_recv,
    head_send,
    head_recv,
    own_sem,
):
    rows = q_ref.shape[1]
    half = rows // 2
    chunks = rows // LANES
    tile = 256 if rows % 256 == 0 else rows
    tokens = normed_ref.shape[0]
    experts = gate_w.shape[0]
    own_hidden = gate_w.shape[1]
    slot_count = picked.shape[0]
    slot_tile = 256 if slot_count % 256 == 0 else slot_count
    slot_span = -(-slot_count // LANES) * LANES

    me = lax.axis_index("ep")
    ep_count = lax.axis_size("ep")
    chips = ep_count // CORES
    chip = me // CORES
    core = me % CORES
    other = 1 - core
    tp_count = lax.axis_size("tp")
    tp_me = lax.axis_index("tp")
    wide, tall = plane_shape(tp_count)
    x_me = tp_me % wide
    y_me = tp_me // wide
    up_hops = chips // 2
    down_hops = chips - 1 - up_hops
    last_down = chips - 2 - up_hops
    features = normed_ref.shape[1] // wide

    def ep_at(turn):
        return lax.rem(me + turn + 1, ep_count)

    def tp_at(turn):
        return lax.rem(tp_me + turn + 1, tp_count)

    def x_at(turn):
        return lax.rem(x_me + turn + 1, wide)

    def y_at(turn):
        return lax.rem(y_me + turn + 1, tall)

    barrier = pltpu.get_barrier_semaphore()

    def greet(**where):
        pl.semaphore_signal(barrier, inc=1, device_id=where)

    loop(ep_count - 1, lambda turn: greet(ep=ep_at(turn)))
    loop(tp_count - 1, lambda turn: greet(tp=tp_at(turn)))

    def room_of(index):
        return pl.ds(pl.multiple_of(index * room, 8), room)

    def feature_lanes(index):
        return pl.ds(pl.multiple_of(index * features, LANES), features)

    piece_lanes = pl.ds(pl.multiple_of(x_me * features + y_me * LANES, LANES), LANES)
    column = lax.broadcasted_iota(jnp.int32, (tokens, LANES), 1)
    marker = jnp.where(column == 0, 1.0, 0.0).astype(jnp.bfloat16)
    ranks = jnp.concatenate([ranks_ref[...], marker], axis=1)
    own_piece = normed_ref[:, piece_lanes]
    for start in range(0, slot_count, slot_tile):
        span = slice(start, start + slot_tile)
        match = dot_nt(places_ref[span, :], ranks)
        pick = jnp.where(match == 0.0, 1.0, 0.0).astype(jnp.bfloat16)
        rows_of = dot(pick, own_piece).astype(jnp.bfloat16)
        picked[span, :] = rows_of

    acc[...] = jnp.zeros_like(acc)
    row_max[...] = jnp.full_like(row_max, neg_fill)

    pl.semaphore_wait(barrier, ep_count + tp_count - 2)

    def pick_copy(target, owner):
        return pltpu.make_async_remote_copy(
            src_ref=picked.at[room_of(target)],
            dst_ref=pieces.at[y_me, room_of(owner)],
            send_sem=pick_send.at[target],
            recv_sem=pick_recv.at[owner],
            device_id={"ep": target},
        )

    def weight_copy(source, index, target, owner):
        return pltpu.make_async_remote_copy(
            src_ref=source.at[:, :, feature_lanes(target)],
            dst_ref=weights.at[owner, index],
            send_sem=weight_send.at[index, target],
            recv_sem=weight_recv.at[index, owner],
            device_id={"tp": y_me * wide + target},
        )

    def own_weight(source, index):
        return pltpu.make_async_copy(
            source.at[:, :, feature_lanes(x_me)], weights.at[x_me, index], own_sem.at[index]
        )

    def up_copy(src, slot):
        return pltpu.make_async_remote_copy(
            src_ref=src,
            dst_ref=held.at[slot],
            send_sem=up_send.at[slot],
            recv_sem=kv_recv.at[slot],
            device_id={"ep": me + CORES},
        )

    def down_copy(src, slot):
        return pltpu.make_async_remote_copy(
            src_ref=src,
            dst_ref=held.at[slot],
            send_sem=down_send.at[slot],
            recv_sem=kv_recv.at[slot],
            device_id={"ep": lax.rem(chip + chips - 1, chips) * CORES + core},
        )

    def side_copy(src, slot):
        return pltpu.make_async_remote_copy(
            src_ref=src,
            dst_ref=held.at[slot],
            send_sem=side_send.at[slot],
            recv_sem=kv_recv.at[slot],
            device_id={"ep": chip * CORES + other},
        )

    def piece_copy(target, owner):
        return pltpu.make_async_remote_copy(
            src_ref=pieces.at[owner],
            dst_ref=pieces.at[owner],
            send_sem=piece_send.at[target],
            recv_sem=piece_recv.at[owner],
            device_id={"tp": target * wide + x_me},
        )

    def part_copy(target, owner):
        return pltpu.make_async_remote_copy(
            src_ref=part_out.at[target],
            dst_ref=part_in.at[owner],
            send_sem=part_send.at[target],
            recv_sem=part_recv.at[owner],
            device_id={"tp": y_me * wide + target},
        )

    def hidden_copy(target, owner):
        return pltpu.make_async_remote_copy(
            src_ref=hidden_out,
            dst_ref=hidden_all.at[owner],
            send_sem=hidden_send.at[target],
            recv_sem=hidden_recv.at[owner],
            device_id={"tp": target},
        )

    def result_copy(target, owner):
        return pltpu.make_async_remote_copy(
            src_ref=result_out.at[room_of(target)],
            dst_ref=result_in.at[room_of(owner)],
            send_sem=result_send.at[target],
            recv_sem=result_recv.at[owner],
            device_id={"ep": target},
        )

    def own_result():
        return pltpu.make_async_copy(
            result_out.at[room_of(me)], result_in.at[room_of(me)], own_sem.at[2]
        )

    def head_copy(target, owner):
        return pltpu.make_async_remote_copy(
            src_ref=heads_out,
            dst_ref=heads_all.at[owner],
            send_sem=head_send.at[target],
            recv_sem=head_recv.at[owner],
            device_id={"tp": target},
        )

    def own_pick():
        return pltpu.make_async_copy(
            picked.at[room_of(me)], pieces.at[y_me, room_of(me)], own_sem.at[3]
        )

    loop(ep_count - 1, lambda turn: pick_copy(ep_at(turn), me).start())
    own_pick().start()

    @pl.when(chip < chips - 1)
    def _():
        up_copy(kv_ref, me).start()

    @pl.when(chip <= last_down)
    def _():
        down_copy(kv_ref, me).start()

    @pl.when(core == 0)
    def _():
        side_copy(kv_ref, me).start()

    def start_weights(turn):
        weight_copy(gate_w, 0, x_at(turn), x_me).start()
        weight_copy(up_w, 1, x_at(turn), x_me).start()

    loop(wide - 1, start_weights)
    own_weight(gate_w, 0).start()
    own_weight(up_w, 1).start()

    ones = jnp.ones((acc.shape[0] - HEAD, rows), jnp.bfloat16)
    nothing = jnp.zeros((HEAD, tile), jnp.bfloat16)

    def block_step(block, source, masked):
        mark = lax.broadcasted_iota(jnp.int32, (LANES, tile), 0)
        wanted = jnp.logical_and(mark // TERMS == block, mark % TERMS < TERMS - 1)
        chosen = jnp.where(wanted, 1.0, 0.0).astype(jnp.bfloat16)
        keys = source[0:half, :]
        early = jnp.concatenate([keys, terms_ref[0:half, :]], axis=1)
        late = jnp.concatenate([keys, terms_ref[half:rows, :]], axis=1)
        values = jnp.concatenate(
            [source[half + HEAD * i : half + HEAD * (i + 1), :] for i in range(chunks)], axis=1
        )
        values = jnp.concatenate([values, ones], axis=0)
        for start in range(0, rows, tile):
            span = slice(start, start + tile)
            query = q_ref[:, span]
            first = dot(early, jnp.concatenate([query, nothing, chosen], axis=0))
            second = dot(late, jnp.concatenate([nothing, query, chosen], axis=0))
            if masked:
                q_pos = start + lax.broadcasted_iota(jnp.int32, first.shape, 1)
                k_pos = lax.broadcasted_iota(jnp.int32, first.shape, 0)
                first = jnp.where(k_pos <= q_pos, first, neg_fill)
                second = jnp.where(k_pos + half <= q_pos, second, neg_fill)
            old_max = row_max[0:1, span]
            top = jnp.maximum(
                jnp.max(first, axis=0, keepdims=True), jnp.max(second, axis=0, keepdims=True)
            )
            new_max = jnp.maximum(old_max, top)
            probs = jnp.concatenate(
                [
                    jnp.exp2((first - new_max) * LOG2E).astype(jnp.bfloat16),
                    jnp.exp2((second - new_max) * LOG2E).astype(jnp.bfloat16),
                ],
                axis=0,
            )
            keep = jnp.exp2((old_max - new_max) * LOG2E)
            acc[:, span] = acc[:, span] * keep + dot(values, probs)
            row_max[0:1, span] = new_max

    block_step(me, kv_ref, True)

    high = weight_ref[...].astype(jnp.bfloat16)
    low = (weight_ref[...] - high.astype(jnp.float32)).astype(jnp.bfloat16)
    for start in range(0, slot_count, slot_tile):
        span = slice(start, start + slot_tile)
        match = dot_nt(ranks, places_ref[span, :])
        for index, part in enumerate((high, low)):
            value = dot_nt(part, places_ref[span, 0:LANES])
            spread[index, :, span] = jnp.where(match == 0.0, value, 0.0).astype(jnp.bfloat16)
    shared = silu(dot_nt(shared_gate_ref[...], normed_ref[...])) * dot_nt(
        shared_up_ref[...], normed_ref[...]
    )
    hidden_out[...] = jnp.zeros_like(hidden_out)
    hidden_out[:, slot_span : slot_span + tokens] = shared.astype(jnp.bfloat16)

    def choose(parts, span):
        owner = owner_ref[0:1, span]
        value = parts[0]
        for index in range(1, experts):
            value = jnp.where(owner == float(index), parts[index], value)
        return value

    def gather_stage():
        loop(ep_count - 1, lambda turn: pick_copy(ep_at(turn), ep_at(turn)).wait_recv())
        own_pick().wait()
        loop(tall - 1, lambda turn: piece_copy(y_at(turn), y_me).start())

    def parts_stage():
        loop(tall - 1, lambda turn: piece_copy(y_at(turn), y_at(turn)).wait_recv())

        def wait_weights(turn):
            weight_copy(gate_w, 0, x_at(turn), x_at(turn)).wait_recv()
            weight_copy(up_w, 1, x_at(turn), x_at(turn)).wait_recv()

        loop(wide - 1, wait_weights)
        own_weight(gate_w, 0).wait()
        own_weight(up_w, 1).wait()

        def one_target(turn):
            target = lax.rem(x_me + turn, wide)
            block = weights[target].reshape(2 * experts * own_hidden, features)
            for start in range(0, slot_count, slot_tile):
                span = slice(start, start + slot_tile)
                rows_of = jnp.concatenate([pieces[y, span, :] for y in range(tall)], axis=1)
                full = dot_nt(block, rows_of)
                halves = []
                for index in range(2):
                    base = index * experts * own_hidden
                    halves.append(
                        choose(
                            [
                                full[base + e * own_hidden : base + (e + 1) * own_hidden]
                                for e in range(experts)
                            ],
                            span,
                        )
                    )
                part_out[target, :, span] = jnp.concatenate(halves, axis=0).astype(jnp.bfloat16)

        loop(wide, one_target)
        loop(wide - 1, lambda turn: part_copy(x_at(turn), x_me).start())

    def hidden_stage():
        loop(wide - 1, lambda turn: part_copy(x_at(turn), x_at(turn)).wait_recv())
        total = part_out[x_me].astype(jnp.float32)
        for turn in range(wide - 1):
            total = total + part_in[x_at(turn)].astype(jnp.float32)
        hidden = silu(total[0:own_hidden]) * total[own_hidden:]
        hidden_out[:, 0:slot_count] = hidden.astype(jnp.bfloat16)
        hidden_all[tp_me] = hidden_out[...]
        loop(tp_count - 1, lambda turn: hidden_copy(tp_at(turn), tp_me).start())

    def down_stage():
        loop(tp_count - 1, lambda turn: hidden_copy(tp_at(turn), tp_at(turn)).wait_recv())
        for start in range(0, slot_count, slot_tile):
            span = slice(start, start + slot_tile)
            units = hidden_all[:, :, span].reshape(tp_count * own_hidden, slot_tile)
            results = [dot(down_ref[e], units) for e in range(experts)]
            result_out[span, :] = choose(results, span).T.astype(jnp.bfloat16)
        loop(ep_count - 1, lambda turn: result_copy(ep_at(turn), me).start())
        own_result().start()

    def received(hop, downward):
        going_up = jnp.logical_and(hop >= 1, jnp.logical_and(hop <= up_hops, chip - hop >= 0))
        source = lax.rem(chip + hop, chips)
        going_down = jnp.logical_and(
            hop >= 1, jnp.logical_and(hop <= down_hops, source <= last_down)
        )
        return jnp.where(downward, going_down, going_up)

    def useful(hop, downward):
        return jnp.logical_and(
            received(hop, downward), jnp.logical_or(jnp.logical_not(downward), chip + hop >= chips)
        )

    def forwards_up(hop):
        return jnp.logical_and(
            received(hop, False), jnp.logical_and(hop < up_hops, chip < chips - 1)
        )

    def forwards_down(hop):
        return jnp.logical_and(received(hop, True), hop < down_hops)

    def home_of(hop, downward):
        return jnp.where(downward, lax.rem(chip + hop, chips), chip - hop)

    def substep(index):
        hop = index // 4
        kind = index % 4
        downward = kind % 2 == 1
        own_core = kind < 2
        home = home_of(hop, downward)
        slot = home * CORES + jnp.where(own_core, core, other)
        sibling = jnp.logical_and(index == 2, core == 1)
        used = useful(hop, downward)

        @pl.when(jnp.logical_and(own_core, received(hop, downward)))
        def _():
            up_copy(held.at[slot], slot).wait_recv()

        @pl.when(jnp.logical_and(kind == 0, forwards_up(hop)))
        def _():
            up_copy(held.at[slot], slot).start()

        @pl.when(jnp.logical_and(kind == 1, forwards_down(hop)))
        def _():
            down_copy(held.at[slot], slot).start()

        @pl.when(jnp.logical_and(own_core, used))
        def _():
            side_copy(held.at[slot], slot).start()

        @pl.when(jnp.logical_or(jnp.logical_and(jnp.logical_not(own_core), used), sibling))
        def _():
            side_copy(held.at[slot], slot).wait_recv()

        @pl.when(jnp.logical_or(used, sibling))
        def _():
            block_step(slot, held.at[slot], False)

        pl.when(index == GATHER_AT)(gather_stage)
        pl.when(index == PARTS_AT)(parts_stage)
        pl.when(index == HIDDEN_AT)(hidden_stage)
        pl.when(index == DOWN_AT)(down_stage)

    loop(max(4 * up_hops + 4, DOWN_AT + 1), substep, 2)

    heads_out[...] = (acc[0:HEAD] / acc[HEAD : HEAD + 1]).astype(jnp.bfloat16)
    heads_all[tp_me] = heads_out[...]
    loop(tp_count - 1, lambda turn: head_copy(tp_at(turn), tp_me).start())

    loop(ep_count - 1, lambda turn: result_copy(ep_at(turn), ep_at(turn)).wait_recv())
    own_result().wait()
    shared_units = hidden_all[:, :, slot_span:].reshape(tp_count * own_hidden, -1)
    shared_sum = dot(shared_down_ref[...], shared_units).T[0:tokens]
    routed = dot(spread[0], result_in[...]) + dot(spread[1], result_in[...])
    moe_ref[...] = (routed + shared_sum).astype(moe_ref.dtype)

    def finish_ep(turn):
        pick_copy(ep_at(turn), me).wait_send()
        result_copy(ep_at(turn), me).wait_send()

    loop(ep_count - 1, finish_ep)
    loop(tall - 1, lambda turn: piece_copy(y_at(turn), y_me).wait_send())

    def finish_x(turn):
        weight_copy(gate_w, 0, x_at(turn), x_me).wait_send()
        weight_copy(up_w, 1, x_at(turn), x_me).wait_send()
        part_copy(x_at(turn), x_me).wait_send()

    loop(wide - 1, finish_x)
    loop(tp_count - 1, lambda turn: hidden_copy(tp_at(turn), tp_me).wait_send())

    @pl.when(chip < chips - 1)
    def _():
        up_copy(kv_ref, me).wait_send()

    @pl.when(chip <= last_down)
    def _():
        down_copy(kv_ref, me).wait_send()

    @pl.when(core == 0)
    def _():
        side_copy(kv_ref, me).wait_send()

    def finish_hop(hop):
        low_slot = home_of(hop, False) * CORES + core
        high_slot = home_of(hop, True) * CORES + core

        @pl.when(forwards_up(hop))
        def _():
            up_copy(held.at[low_slot], low_slot).wait_send()

        @pl.when(forwards_down(hop))
        def _():
            down_copy(held.at[high_slot], high_slot).wait_send()

        @pl.when(useful(hop, False))
        def _():
            side_copy(held.at[low_slot], low_slot).wait_send()

        @pl.when(useful(hop, True))
        def _():
            side_copy(held.at[high_slot], high_slot).wait_send()

    loop(up_hops + 1, finish_hop, 1)

    loop(tp_count - 1, lambda turn: head_copy(tp_at(turn), tp_at(turn)).wait_recv())
    for start in range(0, rows, tile):
        span = slice(start, start + tile)
        units = heads_all[:, :, span].reshape(tp_count * HEAD, tile)
        mixed = dot(out_weight_ref[...], units)
        mixer_ref[span, :] = mixed.T.astype(mixer_ref.dtype)
    loop(tp_count - 1, lambda turn: head_copy(tp_at(turn), tp_me).wait_send())


def slot_tables(ep_count, experts, cap, room):
    slot = np.arange(ep_count * room)
    inside = slot % room
    real = inside < experts * cap
    places = np.zeros((slot.size, 2 * LANES), np.float32)
    expert = (slot // room) * experts + inside // cap
    places[slot[real], expert[real]] = 1.0
    places[:, LANES] = np.where(real, -(inside % cap), 5.0)
    owner = np.where(real, inside // cap, 0).astype(np.float32)
    return jnp.asarray(places, jnp.bfloat16), jnp.asarray(np.tile(owner, (8, 1)), jnp.float32)


def local(
    query_rows,
    key_rows,
    value_rows,
    cum_gate,
    out_weight,
    moe_input,
    moe_gain,
    routes,
    route_weight,
    expert_gate,
    expert_up,
    expert_down,
    shared_gate,
    shared_up,
    shared_down,
):
    rows, width = query_rows.shape
    half = rows // 2
    chunks = rows // LANES
    token_count = moe_input.shape[0]
    top_count = routes.shape[1]
    experts, model, own_hidden = expert_gate.shape
    ep_count = lax.axis_size("ep")
    tp_count = lax.axis_size("tp")
    wide, tall = plane_shape(tp_count)
    expert_count = experts * ep_count
    cap = 2 * token_count * top_count // expert_count
    room = -(-experts * cap // 8) * 8
    slot_count = ep_count * room
    slot_span = -(-slot_count // LANES) * LANES
    hidden_span = slot_span + -(-token_count // LANES) * LANES
    columns = expert_down.shape[2]

    moe_rows = moe_input.astype(jnp.float32)
    normed = (
        moe_rows
        * lax.rsqrt(jnp.mean(moe_rows * moe_rows, axis=1, keepdims=True) + norm_eps)
        * moe_gain
    ).astype(jnp.bfloat16)
    expert_ids = jnp.arange(LANES, dtype=jnp.int32)
    chosen = routes[:, :, None] == expert_ids[None, None, :]
    named = jnp.any(chosen, axis=1)
    weight_of = jnp.sum(jnp.where(chosen, route_weight[:, :, None], 0.0), axis=1)
    order = jnp.arange(token_count)
    earlier = (order[None, :] < order[:, None]).astype(jnp.bfloat16)
    ranks = jnp.dot(earlier, named.astype(jnp.bfloat16), preferred_element_type=jnp.float32)
    ranks = jnp.where(named, ranks, -1.0).astype(jnp.bfloat16)

    queries = query_rows.T * jnp.asarray(HEAD**-0.5, jnp.bfloat16)
    value_cols = value_rows.T
    key_value = jnp.concatenate(
        [jnp.concatenate([key_rows[:half], key_rows[half:]], axis=1)]
        + [value_cols[:, LANES * i : LANES * (i + 1)] for i in range(chunks)],
        axis=0,
    )
    minus = -cum_gate.reshape(ep_count, rows)
    first = lax.reduce_precision(minus, 8, 7)
    rest = minus - first
    second = lax.reduce_precision(rest, 8, 7)
    third = rest - second
    terms = jnp.stack([first, second, third, jnp.zeros_like(third)], axis=1).astype(jnp.bfloat16)
    terms = terms.reshape(ep_count * TERMS, rows)
    terms = jnp.pad(terms, ((0, LANES - ep_count * TERMS), (0, 0))).T

    places, owner = slot_tables(ep_count, experts, cap, room)
    dma = pltpu.SemaphoreType.DMA
    vmem = pl.BlockSpec(memory_space=pltpu.VMEM)
    anywhere = pl.BlockSpec(memory_space=pl.ANY)
    blocks = ep_count * rows * rows
    bf16 = jnp.bfloat16
    mixer_out, moe_out = pl.pallas_call(
        functools.partial(layer_kernel, cap, room),
        out_shape=[
            jax.ShapeDtypeStruct((rows, columns), bf16),
            jax.ShapeDtypeStruct((token_count, columns), bf16),
        ],
        in_specs=[vmem] * 8 + [anywhere] * 2 + [vmem] * 5,
        out_specs=[vmem, vmem],
        scratch_shapes=[
            pltpu.VMEM((ep_count, rows, LANES), bf16),
            pltpu.VMEM((HEAD + 16, rows), jnp.float32),
            pltpu.VMEM((8, rows), jnp.float32),
            pltpu.VMEM((slot_count, LANES), bf16),
            pltpu.VMEM((tall, slot_count, LANES), bf16),
            pltpu.VMEM((wide, 2, experts, own_hidden, model // wide), bf16),
            pltpu.VMEM((wide, 2 * own_hidden, slot_count), bf16),
            pltpu.VMEM((wide, 2 * own_hidden, slot_count), bf16),
            pltpu.VMEM((own_hidden, hidden_span), bf16),
            pltpu.VMEM((tp_count, own_hidden, hidden_span), bf16),
            pltpu.VMEM((slot_count, columns), bf16),
            pltpu.VMEM((slot_count, columns), bf16),
            pltpu.VMEM((2, token_count, slot_count), bf16),
            pltpu.VMEM((HEAD, rows), bf16),
            pltpu.VMEM((tp_count, HEAD, rows), bf16),
        ]
        + [dma((ep_count,))] * 8
        + [dma((tall,))] * 2
        + [dma((2, wide))] * 2
        + [dma((wide,))] * 2
        + [dma((tp_count,))] * 4
        + [dma((4,))],
        compiler_params=pltpu.CompilerParams(
            collective_id=0, has_side_effects=True, vmem_limit_bytes=56 * 1024 * 1024
        ),
        cost_estimate=pl.CostEstimate(
            flops=blocks * 2 * 512, bytes_accessed=8 * 1024 * 1024, transcendentals=blocks
        ),
        name="layer",
    )(
        queries,
        key_value,
        terms,
        normed,
        ranks,
        weight_of,
        places,
        owner,
        expert_gate.transpose(0, 2, 1),
        expert_up.transpose(0, 2, 1),
        expert_down.transpose(0, 2, 1),
        shared_gate.T,
        shared_up.T,
        shared_down.T,
        out_weight.T,
    )
    return mixer_out, moe_out


def solution(mesh):
    placed = (
        P("ep", "tp"),
        P("ep", "tp"),
        P("ep", "tp"),
        P("tp", None),
        P(None, "tp"),
        P("ep", None),
        P(),
        P("ep", None),
        P("ep", None),
        P("ep", None, "tp"),
        P("ep", None, "tp"),
        P("ep", None, "tp"),
        P(None, "tp"),
        P(None, "tp"),
        P(None, "tp"),
    )
    return jax.shard_map(
        local, mesh=mesh, in_specs=placed, out_specs=(P("ep", "tp"), P("ep", "tp")), check_vma=False
    )
```

```python
import functools

import jax
import jax.numpy as jnp
import numpy as np
from jax import lax
from jax.experimental import pallas as pl
from jax.experimental.pallas import tpu as pltpu
from jax.sharding import PartitionSpec as P

HEAD = 64
LANES = 128
CORES = 2
TERMS = 4
LOG2E = 1.4426950408889634

neg_fill = -1e30
norm_eps = 1e-06

NEAR_AT = 7
FAR_AT = 9
PARTS_AT = 17
HIDDEN_AT = 24
DOWN_AT = 27
RETURN_AT = 31


def plane_shape(tp_count):
    wide = 1
    while wide * wide < tp_count:
        wide *= 2
    return wide, tp_count // wide


def dot(a, b):
    return jnp.dot(a, b, preferred_element_type=jnp.float32)


def dot_nt(a, b):
    return lax.dot_general(a, b, (((1,), (1,)), ((), ())), preferred_element_type=jnp.float32)


def silu(v):
    return v / (1.0 + jnp.exp(-v))


def loop(count, body, first=0):
    def step(index, carry):
        body(index)
        return carry

    lax.fori_loop(first, count, step, 0)


def layer_kernel(
    cap,
    room,
    q_ref,
    kv_ref,
    terms_ref,
    normed_ref,
    ranks_ref,
    weight_ref,
    places_ref,
    owner_ref,
    gate_w,
    up_w,
    down_w,
    shared_gate_ref,
    shared_up_ref,
    shared_down_ref,
    out_weight_ref,
    mixer_ref,
    moe_ref,
    held,
    acc,
    row_max,
    picked,
    pieces,
    weights,
    down_all,
    part_out,
    part_in,
    hidden_all,
    shared_out,
    shared_all,
    result_out,
    result_all,
    result_in,
    spread,
    heads_all,
    up_send,
    down_send,
    side_send,
    kv_recv,
    pick_send,
    pick_recv,
    result_send,
    result_recv,
    cross_send,
    cross_recv,
    piece_send,
    piece_recv,
    weight_send,
    weight_recv,
    part_send,
    part_recv,
    hidden_send,
    hidden_recv,
    shared_send,
    shared_recv,
    row_send,
    column_send,
    head_recv,
    own_sem,
):
    rows = q_ref.shape[1]
    half = rows // 2
    chunks = rows // LANES
    tile = 256 if rows % 256 == 0 else rows
    tokens = normed_ref.shape[0]
    experts = gate_w.shape[0]
    own_hidden = gate_w.shape[1]
    slot_count = picked.shape[0]
    slot_tile = 256 if slot_count % 256 == 0 else slot_count

    me = lax.axis_index("ep")
    ep_count = lax.axis_size("ep")
    chips = ep_count // CORES
    chip = me // CORES
    core = me % CORES
    other = 1 - core
    tp_count = lax.axis_size("tp")
    tp_me = lax.axis_index("tp")
    wide, tall = plane_shape(tp_count)
    x_me = tp_me % wide
    y_me = tp_me // wide
    up_hops = chips // 2
    down_hops = chips - 1 - up_hops
    last_down = chips - 2 - up_hops
    features = normed_ref.shape[1] // wide
    share = ep_count // wide
    share_rows = share * room
    keeper = me // share

    def ep_at(turn):
        return lax.rem(me + turn + 1, ep_count)

    def tp_at(turn):
        return lax.rem(tp_me + turn + 1, tp_count)

    def x_at(turn):
        return lax.rem(x_me + turn + 1, wide)

    def y_at(turn):
        return lax.rem(y_me + turn + 1, tall)

    barrier = pltpu.get_barrier_semaphore()

    def greet(**where):
        pl.semaphore_signal(barrier, inc=1, device_id=where)

    loop(ep_count - 1, lambda turn: greet(ep=ep_at(turn)))
    loop(tp_count - 1, lambda turn: greet(tp=tp_at(turn)))

    def room_of(index):
        return pl.ds(pl.multiple_of(index * room, 8), room)

    def feature_lanes(index):
        return pl.ds(pl.multiple_of(index * features, LANES), features)

    piece_lanes = pl.ds(pl.multiple_of(x_me * features + y_me * LANES, LANES), LANES)
    column = lax.broadcasted_iota(jnp.int32, (tokens, LANES), 1)
    marker = jnp.where(column == 0, 1.0, 0.0).astype(jnp.bfloat16)
    ranks = jnp.concatenate([ranks_ref[...], marker], axis=1)
    own_piece = normed_ref[:, piece_lanes]
    for start in range(0, slot_count, slot_tile):
        span = slice(start, start + slot_tile)
        match = dot_nt(places_ref[span, :], ranks)
        pick = jnp.where(match == 0.0, 1.0, 0.0).astype(jnp.bfloat16)
        rows_of = dot(pick, own_piece).astype(jnp.bfloat16)
        picked[span, :] = rows_of

    acc[...] = jnp.zeros_like(acc)
    row_max[...] = jnp.full_like(row_max, neg_fill)

    pl.semaphore_wait(barrier, ep_count + tp_count - 2)

    def pick_copy(target, owner):
        return pltpu.make_async_remote_copy(
            src_ref=picked.at[room_of(target)],
            dst_ref=pieces.at[y_me, room_of(owner)],
            send_sem=pick_send.at[target],
            recv_sem=pick_recv.at[owner],
            device_id={"ep": target},
        )

    sources = (
        (gate_w.at[:, :, feature_lanes(x_me)], lambda owner: weights.at[0, :, owner]),
        (up_w.at[:, :, feature_lanes(x_me)], lambda owner: weights.at[1, :, owner]),
        (down_w, lambda owner: down_all.at[owner]),
    )

    def weight_copy(index, target, owner):
        source = down_w
        if index < 2:
            source = (gate_w, up_w)[index].at[:, :, feature_lanes(target)]
        return pltpu.make_async_remote_copy(
            src_ref=source,
            dst_ref=sources[index][1](owner),
            send_sem=weight_send.at[index, target],
            recv_sem=weight_recv.at[index, owner],
            device_id={"tp": y_me * wide + target},
        )

    def own_weight(index):
        return pltpu.make_async_copy(
            sources[index][0], sources[index][1](x_me), own_sem.at[index]
        )

    def up_copy(src, slot):
        return pltpu.make_async_remote_copy(
            src_ref=src,
            dst_ref=held.at[slot],
            send_sem=up_send.at[slot],
            recv_sem=kv_recv.at[slot],
            device_id={"ep": me + CORES},
        )

    def down_copy(src, slot):
        return pltpu.make_async_remote_copy(
            src_ref=src,
            dst_ref=held.at[slot],
            send_sem=down_send.at[slot],
            recv_sem=kv_recv.at[slot],
            device_id={"ep": lax.rem(chip + chips - 1, chips) * CORES + core},
        )

    def side_copy(src, slot):
        return pltpu.make_async_remote_copy(
            src_ref=src,
            dst_ref=held.at[slot],
            send_sem=side_send.at[slot],
            recv_sem=kv_recv.at[slot],
            device_id={"ep": chip * CORES + other},
        )

    def piece_copy(group, target, owner):
        place = pieces.at[owner, pl.ds(pl.multiple_of(group * share_rows, 8), share_rows)]
        return pltpu.make_async_remote_copy(
            src_ref=place,
            dst_ref=place,
            send_sem=piece_send.at[target, group],
            recv_sem=piece_recv.at[owner, group],
            device_id={"tp": target * wide + x_me},
        )

    def part_copy(target, owner):
        return pltpu.make_async_remote_copy(
            src_ref=part_out.at[pl.ds(pl.multiple_of(target * share_rows, 8), share_rows)],
            dst_ref=part_in.at[owner],
            send_sem=part_send.at[target],
            recv_sem=part_recv.at[owner],
            device_id={"tp": y_me * wide + target},
        )

    def hidden_copy(target, owner):
        return pltpu.make_async_remote_copy(
            src_ref=hidden_all.at[owner],
            dst_ref=hidden_all.at[owner],
            send_sem=hidden_send.at[target],
            recv_sem=hidden_recv.at[owner],
            device_id={"tp": target * wide + x_me},
        )

    def shared_copy(target, owner):
        return pltpu.make_async_remote_copy(
            src_ref=shared_out,
            dst_ref=shared_all.at[owner],
            send_sem=shared_send.at[target],
            recv_sem=shared_recv.at[owner],
            device_id={"tp": target},
        )

    def share_of(index):
        return pl.ds(pl.multiple_of(index * share_rows, 8), share_rows)

    def cross_copy(target, owner):
        return pltpu.make_async_remote_copy(
            src_ref=result_out.at[target],
            dst_ref=result_all.at[share_of(owner)],
            send_sem=cross_send.at[target],
            recv_sem=cross_recv.at[owner],
            device_id={"tp": y_me * wide + target},
        )

    def own_cross():
        return pltpu.make_async_copy(
            result_out.at[x_me], result_all.at[share_of(x_me)], own_sem.at[5]
        )

    def result_copy(target, owner):
        return pltpu.make_async_remote_copy(
            src_ref=result_all.at[room_of(target)],
            dst_ref=result_in.at[room_of(owner)],
            send_sem=result_send.at[target],
            recv_sem=result_recv.at[owner],
            device_id={"ep": target},
        )

    def own_result():
        return pltpu.make_async_copy(
            result_all.at[room_of(me)], result_in.at[room_of(me)], own_sem.at[4]
        )

    half_head = HEAD // 2

    def row_copy(owner_y, owner_x, part, target, sem):
        place = heads_all.at[owner_y, owner_x, part * half_head : (part + 1) * half_head]
        return pltpu.make_async_remote_copy(
            src_ref=place,
            dst_ref=place,
            send_sem=sem,
            recv_sem=head_recv.at[part, owner_y * wide + owner_x],
            device_id={"tp": y_me * wide + target},
        )

    def column_copy(owner_y, owner_x, part, target, sem):
        place = heads_all.at[owner_y, owner_x, part * half_head : (part + 1) * half_head]
        return pltpu.make_async_remote_copy(
            src_ref=place,
            dst_ref=place,
            send_sem=sem,
            recv_sem=head_recv.at[part, owner_y * wide + owner_x],
            device_id={"tp": target * wide + x_me},
        )

    def row_part(owner_x, target):
        return column_copy(y_me, owner_x, 0, target, column_send.at[0, owner_x, target])

    def row_first(target, owner_x):
        return row_copy(y_me, owner_x, 0, target, row_send.at[1, tall, target])

    def column_part(owner_y, target):
        return row_copy(owner_y, x_me, 1, target, row_send.at[0, owner_y, target])

    def column_first(target, owner_y):
        return column_copy(owner_y, x_me, 1, target, column_send.at[1, wide, target])

    def own_pick():
        return pltpu.make_async_copy(
            picked.at[room_of(me)], pieces.at[y_me, room_of(me)], own_sem.at[3]
        )

    @pl.when(chip < chips - 1)
    def _():
        up_copy(kv_ref, me).start()

    @pl.when(chip <= last_down)
    def _():
        down_copy(kv_ref, me).start()

    @pl.when(core == 0)
    def _():
        side_copy(kv_ref, me).start()

    loop(ep_count - 1, lambda turn: pick_copy(ep_at(turn), me).start())
    own_pick().start()

    loop(wide - 1, lambda turn: weight_copy(0, x_at(turn), x_me).start())
    loop(wide - 1, lambda turn: weight_copy(1, x_at(turn), x_me).start())
    for index in range(3):
        own_weight(index).start()
    loop(wide - 1, lambda turn: weight_copy(2, x_at(turn), x_me).start())

    ones = jnp.ones((acc.shape[0] - HEAD, rows), jnp.bfloat16)
    nothing = jnp.zeros((HEAD, tile), jnp.bfloat16)

    def block_step(block, source, masked):
        mark = lax.broadcasted_iota(jnp.int32, (LANES, tile), 0)
        wanted = jnp.logical_and(mark // TERMS == block, mark % TERMS < TERMS - 1)
        chosen = jnp.where(wanted, 1.0, 0.0).astype(jnp.bfloat16)
        keys = source[0:half, :]
        early = jnp.concatenate([keys, terms_ref[0:half, :]], axis=1)
        late = jnp.concatenate([keys, terms_ref[half:rows, :]], axis=1)
        values = jnp.concatenate(
            [source[half + HEAD * i : half + HEAD * (i + 1), :] for i in range(chunks)], axis=1
        )
        values = jnp.concatenate([values, ones], axis=0)
        for start in range(0, rows, tile):
            span = slice(start, start + tile)
            query = q_ref[:, span]
            first = dot(early, jnp.concatenate([query, nothing, chosen], axis=0))
            second = dot(late, jnp.concatenate([nothing, query, chosen], axis=0))
            if masked:
                q_pos = start + lax.broadcasted_iota(jnp.int32, first.shape, 1)
                k_pos = lax.broadcasted_iota(jnp.int32, first.shape, 0)
                first = jnp.where(k_pos <= q_pos, first, neg_fill)
                second = jnp.where(k_pos + half <= q_pos, second, neg_fill)
            old_max = row_max[0:1, span]
            top = jnp.maximum(
                jnp.max(first, axis=0, keepdims=True), jnp.max(second, axis=0, keepdims=True)
            )
            new_max = jnp.maximum(old_max, top)
            probs = jnp.concatenate(
                [
                    jnp.exp2((first - new_max) * LOG2E).astype(jnp.bfloat16),
                    jnp.exp2((second - new_max) * LOG2E).astype(jnp.bfloat16),
                ],
                axis=0,
            )
            keep = jnp.exp2((old_max - new_max) * LOG2E)
            acc[:, span] = acc[:, span] * keep + dot(values, probs)
            row_max[0:1, span] = new_max

    block_step(me, kv_ref, True)

    high = weight_ref[...].astype(jnp.bfloat16)
    low = (weight_ref[...] - high.astype(jnp.float32)).astype(jnp.bfloat16)
    for start in range(0, slot_count, slot_tile):
        span = slice(start, start + slot_tile)
        match = dot_nt(ranks, places_ref[span, :])
        for index, part in enumerate((high, low)):
            value = dot_nt(part, places_ref[span, 0:LANES])
            spread[index, :, span] = jnp.where(match == 0.0, value, 0.0).astype(jnp.bfloat16)
    shared = silu(dot_nt(shared_gate_ref[...], normed_ref[...])) * dot_nt(
        shared_up_ref[...], normed_ref[...]
    )
    shared_out[...] = jnp.zeros_like(shared_out)
    shared_out[:, 0:tokens] = shared.astype(jnp.bfloat16)
    shared_all[tp_me] = shared_out[...]
    loop(tp_count - 1, lambda turn: shared_copy(tp_at(turn), tp_me).start())

    def choose(parts, span):
        owner = owner_ref[span, 0:1]
        value = parts[0]
        for index in range(1, experts):
            value = jnp.where(owner == float(index), parts[index], value)
        return value

    def forward_group(group):
        def wait_block(turn):
            source = group * share + turn

            @pl.when(source != me)
            def _():
                pick_copy(source, source).wait_recv()

        loop(share, wait_block)
        loop(tall - 1, lambda turn: piece_copy(group, y_at(turn), y_me).start())

    def near_stage():
        own_pick().wait()
        forward_group(keeper)

    def far_stage():
        loop(wide, lambda turn: forward_group(lax.rem(keeper + turn, wide)), 1)

    def parts_stage():
        def wait_pieces(group):
            loop(tall - 1, lambda turn: piece_copy(group, y_at(turn), y_at(turn)).wait_recv())

        loop(wide, wait_pieces)
        for index in range(2):
            loop(wide - 1, lambda turn: weight_copy(index, x_at(turn), x_at(turn)).wait_recv())
            own_weight(index).wait()

        def one_tile(index):
            start = pl.multiple_of(index * slot_tile, slot_tile)
            span = pl.ds(start, slot_tile)
            rows_of = jnp.concatenate([pieces[y, span, :] for y in range(tall)], axis=1)
            parts = []
            for e in range(experts):
                block = jnp.concatenate(
                    [weights[g, e].reshape(wide * own_hidden, features) for g in range(2)], axis=0
                )
                parts.append(dot_nt(rows_of, block))
            part_out[span, :] = choose(parts, span).astype(jnp.bfloat16)

        loop(slot_count // slot_tile, one_tile)
        loop(wide - 1, lambda turn: part_copy(x_at(turn), x_me).start())

    def hidden_stage():
        loop(wide - 1, lambda turn: part_copy(x_at(turn), x_at(turn)).wait_recv())
        own_rows = pl.ds(pl.multiple_of(x_me * share_rows, 8), share_rows)
        total = part_out[own_rows, :].astype(jnp.float32)
        for turn in range(wide - 1):
            total = total + part_in[x_at(turn)].astype(jnp.float32)
        middle = wide * own_hidden
        hidden = silu(total[:, 0:middle]) * total[:, middle:]
        hidden_all[y_me] = hidden.astype(jnp.bfloat16)
        loop(tall - 1, lambda turn: hidden_copy(y_at(turn), y_me).start())

    def down_stage():
        loop(tall - 1, lambda turn: hidden_copy(y_at(turn), y_at(turn)).wait_recv())
        loop(wide - 1, lambda turn: weight_copy(2, x_at(turn), x_at(turn)).wait_recv())
        own_weight(2).wait()
        units = jnp.concatenate([hidden_all[y] for y in range(tall)], axis=1)
        for x in range(0, wide, 2):
            results = [
                dot(units, jnp.concatenate([down_all[x, e], down_all[x + 1, e]], axis=1))
                for e in range(experts)
            ]
            result = choose(results, slice(0, share_rows)).astype(jnp.bfloat16)
            columns = result.shape[1] // 2
            result_out[x] = result[:, 0:columns]
            result_out[x + 1] = result[:, columns:]

        loop(wide - 1, lambda turn: cross_copy(x_at(turn), x_me).start())
        own_cross().start()

    def return_stage():
        loop(wide - 1, lambda turn: cross_copy(x_at(turn), x_at(turn)).wait_recv())
        own_cross().wait()
        loop(ep_count - 1, lambda turn: result_copy(ep_at(turn), me).start())
        own_result().start()

    def received(hop, downward):
        going_up = jnp.logical_and(hop >= 1, jnp.logical_and(hop <= up_hops, chip - hop >= 0))
        source = lax.rem(chip + hop, chips)
        going_down = jnp.logical_and(
            hop >= 1, jnp.logical_and(hop <= down_hops, source <= last_down)
        )
        return jnp.where(downward, going_down, going_up)

    def useful(hop, downward):
        return jnp.logical_and(
            received(hop, downward), jnp.logical_or(jnp.logical_not(downward), chip + hop >= chips)
        )

    def forwards_up(hop):
        return jnp.logical_and(
            received(hop, False), jnp.logical_and(hop < up_hops, chip < chips - 1)
        )

    def forwards_down(hop):
        return jnp.logical_and(received(hop, True), hop < down_hops)

    def home_of(hop, downward):
        return jnp.where(downward, lax.rem(chip + hop, chips), chip - hop)

    def carry_on(hop, downward):
        slot = home_of(hop, downward) * CORES + core

        @pl.when(received(hop, downward))
        def _():
            up_copy(held.at[slot], slot).wait_recv()

        @pl.when(jnp.logical_and(jnp.logical_not(downward), forwards_up(hop)))
        def _():
            up_copy(held.at[slot], slot).start()

        @pl.when(jnp.logical_and(downward, forwards_down(hop)))
        def _():
            down_copy(held.at[slot], slot).start()

        @pl.when(useful(hop, downward))
        def _():
            side_copy(held.at[slot], slot).start()

    def substep(index):
        pl.when(jnp.logical_and(index >= 4, index % 3 != 0))(
            lambda: carry_on((index - 1) // 3, index % 3 == 2)
        )
        hop = index // 4
        kind = index % 4
        downward = kind % 2 == 1
        own_core = kind < 2
        slot = home_of(hop, downward) * CORES + jnp.where(own_core, core, other)
        sibling = jnp.logical_and(index == 2, core == 1)
        used = useful(hop, downward)

        @pl.when(jnp.logical_or(jnp.logical_and(jnp.logical_not(own_core), used), sibling))
        def _():
            side_copy(held.at[slot], slot).wait_recv()

        @pl.when(jnp.logical_or(used, sibling))
        def _():
            block_step(slot, held.at[slot], False)

        pl.when(index == NEAR_AT)(near_stage)
        pl.when(index == FAR_AT)(far_stage)
        pl.when(index == PARTS_AT)(parts_stage)
        pl.when(index == HIDDEN_AT)(hidden_stage)
        pl.when(index == DOWN_AT)(down_stage)
        pl.when(index == RETURN_AT)(return_stage)

    loop(max(4 * up_hops + 4, RETURN_AT + 1), substep, 2)

    heads = acc[0:HEAD] / acc[HEAD : HEAD + 1]
    heads_all[y_me, x_me] = heads.astype(jnp.bfloat16)
    loop(wide - 1, lambda turn: row_first(x_at(turn), x_me).start())
    loop(tall - 1, lambda turn: column_first(y_at(turn), y_me).start())
    loop(tall - 1, lambda turn: row_part(x_me, y_at(turn)).start())
    loop(wide - 1, lambda turn: column_part(y_me, x_at(turn)).start())

    def pass_row(turn):
        row_first(x_at(turn), x_at(turn)).wait_recv()
        loop(tall - 1, lambda way: row_part(x_at(turn), y_at(way)).start())

    def pass_column(turn):
        column_first(y_at(turn), y_at(turn)).wait_recv()
        loop(wide - 1, lambda way: column_part(y_at(turn), x_at(way)).start())

    loop(wide - 1, pass_row)
    loop(tall - 1, pass_column)

    loop(ep_count - 1, lambda turn: result_copy(ep_at(turn), ep_at(turn)).wait_recv())
    own_result().wait()
    loop(tp_count - 1, lambda turn: shared_copy(tp_at(turn), tp_at(turn)).wait_recv())
    shared_units = shared_all[...].reshape(tp_count * own_hidden, -1)
    shared_sum = dot(shared_down_ref[...], shared_units).T[0:tokens]
    routed = dot(spread[0], result_in[...]) + dot(spread[1], result_in[...])
    moe_ref[...] = (routed + shared_sum).astype(moe_ref.dtype)

    def finish_ep(turn):
        pick_copy(ep_at(turn), me).wait_send()
        result_copy(ep_at(turn), me).wait_send()

    loop(ep_count - 1, finish_ep)

    def finish_pieces(group):
        loop(tall - 1, lambda turn: piece_copy(group, y_at(turn), y_me).wait_send())

    loop(wide, finish_pieces)

    def finish_x(turn):
        for index in range(3):
            weight_copy(index, x_at(turn), x_me).wait_send()
        part_copy(x_at(turn), x_me).wait_send()
        cross_copy(x_at(turn), x_me).wait_send()

    loop(wide - 1, finish_x)
    loop(tall - 1, lambda turn: hidden_copy(y_at(turn), y_me).wait_send())
    loop(tp_count - 1, lambda turn: shared_copy(tp_at(turn), tp_me).wait_send())

    @pl.when(chip < chips - 1)
    def _():
        up_copy(kv_ref, me).wait_send()

    @pl.when(chip <= last_down)
    def _():
        down_copy(kv_ref, me).wait_send()

    @pl.when(core == 0)
    def _():
        side_copy(kv_ref, me).wait_send()

    def finish_hop(hop):
        low_slot = home_of(hop, False) * CORES + core
        high_slot = home_of(hop, True) * CORES + core

        @pl.when(forwards_up(hop))
        def _():
            up_copy(held.at[low_slot], low_slot).wait_send()

        @pl.when(forwards_down(hop))
        def _():
            down_copy(held.at[high_slot], high_slot).wait_send()

        @pl.when(useful(hop, False))
        def _():
            side_copy(held.at[low_slot], low_slot).wait_send()

        @pl.when(useful(hop, True))
        def _():
            side_copy(held.at[high_slot], high_slot).wait_send()

    loop(up_hops + 1, finish_hop, 1)

    def wait_far(turn):
        y = y_at(turn)

        def one(way):
            x = lax.rem(x_me + way, wide)
            column_copy(y, x, 0, 0, column_send.at[0, 0, 0]).wait_recv()

        loop(wide, one)

    def wait_wide(turn):
        x = x_at(turn)

        def one(way):
            y = lax.rem(y_me + way, tall)
            row_copy(y, x, 1, 0, row_send.at[0, 0, 0]).wait_recv()

        loop(tall, one)

    loop(tall - 1, wait_far)
    loop(wide - 1, wait_wide)
    for start in range(0, rows, tile):
        span = slice(start, start + tile)
        units = heads_all[:, :, :, span].reshape(tp_count * HEAD, tile)
        mixed = dot(out_weight_ref[...], units)
        mixer_ref[span, :] = mixed.T.astype(mixer_ref.dtype)

    def finish_row(turn):
        row_first(x_at(turn), x_me).wait_send()
        loop(tall, lambda y: column_part(y, x_at(turn)).wait_send())

    def finish_column(turn):
        column_first(y_at(turn), y_me).wait_send()
        loop(wide, lambda x: row_part(x, y_at(turn)).wait_send())

    loop(wide - 1, finish_row)
    loop(tall - 1, finish_column)


def slot_tables(ep_count, experts, cap, room):
    slot = np.arange(ep_count * room)
    inside = slot % room
    real = inside < experts * cap
    places = np.zeros((slot.size, 2 * LANES), np.float32)
    expert = (slot // room) * experts + inside // cap
    places[slot[real], expert[real]] = 1.0
    places[:, LANES] = np.where(real, -(inside % cap), 5.0)
    owner = np.where(real, inside // cap, 0).astype(np.float32)
    owner = np.tile(owner[:, None], (1, LANES))
    return jnp.asarray(places, jnp.bfloat16), jnp.asarray(owner, jnp.float32)


def local(
    query_rows,
    key_rows,
    value_rows,
    cum_gate,
    out_weight,
    moe_input,
    moe_gain,
    routes,
    route_weight,
    expert_gate,
    expert_up,
    expert_down,
    shared_gate,
    shared_up,
    shared_down,
):
    rows, width = query_rows.shape
    half = rows // 2
    chunks = rows // LANES
    token_count = moe_input.shape[0]
    top_count = routes.shape[1]
    experts, model, own_hidden = expert_gate.shape
    ep_count = lax.axis_size("ep")
    tp_count = lax.axis_size("tp")
    wide, tall = plane_shape(tp_count)
    expert_count = experts * ep_count
    cap = 2 * token_count * top_count // expert_count
    room = -(-experts * cap // 8) * 8
    slot_count = ep_count * room
    share_rows = slot_count // wide
    token_span = -(-token_count // LANES) * LANES
    columns = expert_down.shape[2]

    moe_rows = moe_input.astype(jnp.float32)
    normed = (
        moe_rows
        * lax.rsqrt(jnp.mean(moe_rows * moe_rows, axis=1, keepdims=True) + norm_eps)
        * moe_gain
    ).astype(jnp.bfloat16)
    expert_ids = jnp.arange(LANES, dtype=jnp.int32)
    chosen = routes[:, :, None] == expert_ids[None, None, :]
    named = jnp.any(chosen, axis=1)
    weight_of = jnp.sum(jnp.where(chosen, route_weight[:, :, None], 0.0), axis=1)
    order = jnp.arange(token_count)
    earlier = (order[None, :] < order[:, None]).astype(jnp.bfloat16)
    ranks = jnp.dot(earlier, named.astype(jnp.bfloat16), preferred_element_type=jnp.float32)
    ranks = jnp.where(named, ranks, -1.0).astype(jnp.bfloat16)

    queries = query_rows.T * jnp.asarray(HEAD**-0.5, jnp.bfloat16)
    value_cols = value_rows.T
    key_value = jnp.concatenate(
        [jnp.concatenate([key_rows[:half], key_rows[half:]], axis=1)]
        + [value_cols[:, LANES * i : LANES * (i + 1)] for i in range(chunks)],
        axis=0,
    )
    minus = -cum_gate.reshape(ep_count, rows)
    first = lax.reduce_precision(minus, 8, 7)
    rest = minus - first
    second = lax.reduce_precision(rest, 8, 7)
    third = rest - second
    terms = jnp.stack([first, second, third, jnp.zeros_like(third)], axis=1).astype(jnp.bfloat16)
    terms = terms.reshape(ep_count * TERMS, rows)
    terms = jnp.pad(terms, ((0, LANES - ep_count * TERMS), (0, 0))).T

    places, owner = slot_tables(ep_count, experts, cap, room)
    dma = pltpu.SemaphoreType.DMA
    vmem = pl.BlockSpec(memory_space=pltpu.VMEM)
    anywhere = pl.BlockSpec(memory_space=pl.ANY)
    blocks = ep_count * rows * rows
    bf16 = jnp.bfloat16
    mixer_out, moe_out = pl.pallas_call(
        functools.partial(layer_kernel, cap, room),
        out_shape=[
            jax.ShapeDtypeStruct((rows, columns), bf16),
            jax.ShapeDtypeStruct((token_count, columns), bf16),
        ],
        in_specs=[vmem] * 8 + [anywhere] * 3 + [vmem] * 4,
        out_specs=[vmem, vmem],
        scratch_shapes=[
            pltpu.VMEM((ep_count, rows, LANES), bf16),
            pltpu.VMEM((HEAD + 16, rows), jnp.float32),
            pltpu.VMEM((8, rows), jnp.float32),
            pltpu.VMEM((slot_count, LANES), bf16),
            pltpu.VMEM((tall, slot_count, LANES), bf16),
            pltpu.VMEM((2, experts, wide, own_hidden, model // wide), bf16),
            pltpu.VMEM((wide, experts, tp_count * own_hidden, columns), bf16),
            pltpu.VMEM((slot_count, 2 * wide * own_hidden), bf16),
            pltpu.VMEM((wide, share_rows, 2 * wide * own_hidden), bf16),
            pltpu.VMEM((tall, share_rows, wide * own_hidden), bf16),
            pltpu.VMEM((own_hidden, token_span), bf16),
            pltpu.VMEM((tp_count, own_hidden, token_span), bf16),
            pltpu.VMEM((wide, share_rows, columns), bf16),
            pltpu.VMEM((slot_count, columns), bf16),
            pltpu.VMEM((slot_count, columns), bf16),
            pltpu.VMEM((2, token_count, slot_count), bf16),
            pltpu.VMEM((tall, wide, HEAD, rows), bf16),
        ]
        + [dma((ep_count,))] * 8
        + [dma((wide,))] * 2
        + [dma((tall, wide))] * 2
        + [dma((3, wide))] * 2
        + [dma((wide,))] * 2
        + [dma((tall,))] * 2
        + [dma((tp_count,))] * 2
        + [dma((2, tall + 1, wide)), dma((2, wide + 1, tall)), dma((2, tp_count))]
        + [dma((6,))],
        compiler_params=pltpu.CompilerParams(
            collective_id=0, has_side_effects=True, vmem_limit_bytes=56 * 1024 * 1024
        ),
        cost_estimate=pl.CostEstimate(
            flops=blocks * 2 * 512, bytes_accessed=8 * 1024 * 1024, transcendentals=blocks
        ),
        name="layer",
    )(
        queries,
        key_value,
        terms,
        normed,
        ranks,
        weight_of,
        places,
        owner,
        expert_gate.transpose(0, 2, 1),
        expert_up.transpose(0, 2, 1),
        expert_down,
        shared_gate.T,
        shared_up.T,
        shared_down.T,
        out_weight.T,
    )
    return mixer_out, moe_out


def solution(mesh):
    placed = (
        P("ep", "tp"),
        P("ep", "tp"),
        P("ep", "tp"),
        P("tp", None),
        P(None, "tp"),
        P("ep", None),
        P(),
        P("ep", None),
        P("ep", None),
        P("ep", None, "tp"),
        P("ep", None, "tp"),
        P("ep", None, "tp"),
        P(None, "tp"),
        P(None, "tp"),
        P(None, "tp"),
    )
    return jax.shard_map(
        local, mesh=mesh, in_specs=placed, out_specs=(P("ep", "tp"), P("ep", "tp")), check_vma=False
    )
```

```python
import functools

import jax
import jax.numpy as jnp
import numpy as np
from jax import lax
from jax.experimental import pallas as pl
from jax.experimental.pallas import tpu as pltpu
from jax.sharding import PartitionSpec as P

HEAD = 64
LANES = 128
CORES = 2
TERMS = 4
LOG2E = 1.4426950408889634

neg_fill = -1e30
norm_eps = 1e-06

LOCAL_AT = 5
NEAR_AT = 7
FAR_AT = 9
PARTS_AT = 17
HIDDEN_AT = 23
DOWN_AT = 26
RETURN_AT = 29


def plane_shape(tp_count):
    wide = 1
    while wide * wide < tp_count:
        wide *= 2
    return wide, tp_count // wide


def dot(a, b):
    return jnp.dot(a, b, preferred_element_type=jnp.float32)


def dot_nt(a, b):
    return lax.dot_general(a, b, (((1,), (1,)), ((), ())), preferred_element_type=jnp.float32)


def silu(v):
    return v / (1.0 + jnp.exp(-v))


def loop(count, body, first=0):
    def step(index, carry):
        body(index)
        return carry

    lax.fori_loop(first, count, step, 0)


def layer_kernel(
    cap,
    room,
    query_ref,
    key_ref,
    value_ref,
    gate_ref,
    input_ref,
    gain_ref,
    routes_ref,
    weight_ref,
    places_ref,
    owner_ref,
    gate_w,
    up_w,
    down_w,
    shared_gate_ref,
    shared_up_ref,
    shared_down_ref,
    out_weight_ref,
    mixer_ref,
    moe_ref,
    q_ref,
    kv_ref,
    terms_ref,
    normed_ref,
    weight_rows,
    rank_rows,
    mix_weight,
    shared_weight,
    held,
    acc,
    row_max,
    picked,
    pieces,
    weights,
    down_all,
    part_out,
    part_in,
    hidden_all,
    shared_out,
    shared_all,
    result_out,
    result_all,
    result_in,
    spread,
    heads_all,
    up_send,
    down_send,
    side_send,
    kv_recv,
    pick_send,
    pick_recv,
    result_send,
    result_recv,
    cross_send,
    cross_recv,
    piece_send,
    piece_recv,
    weight_send,
    weight_recv,
    part_send,
    part_recv,
    hidden_send,
    hidden_recv,
    shared_send,
    shared_recv,
    row_send,
    column_send,
    head_recv,
    own_sem,
):
    rows = q_ref.shape[1]
    half = rows // 2
    chunks = rows // LANES
    tile = 256 if rows % 256 == 0 else rows
    tokens = normed_ref.shape[0]
    experts = gate_w.shape[0]
    own_hidden = gate_w.shape[1]
    slot_count = picked.shape[0]
    slot_tile = 256 if slot_count % 256 == 0 else slot_count

    me = lax.axis_index("ep")
    ep_count = lax.axis_size("ep")
    chips = ep_count // CORES
    chip = me // CORES
    core = me % CORES
    other = 1 - core
    tp_count = lax.axis_size("tp")
    tp_me = lax.axis_index("tp")
    wide, tall = plane_shape(tp_count)
    x_me = tp_me % wide
    y_me = tp_me // wide
    up_hops = chips // 2
    down_hops = chips - 1 - up_hops
    last_down = chips - 2 - up_hops
    features = normed_ref.shape[1] // wide
    share = ep_count // wide
    share_rows = share * room
    keeper = me // share

    def ep_at(turn):
        return lax.rem(me + turn + 1, ep_count)

    def tp_at(turn):
        return lax.rem(tp_me + turn + 1, tp_count)

    def x_at(turn):
        return lax.rem(x_me + turn + 1, wide)

    def y_at(turn):
        return lax.rem(y_me + turn + 1, tall)

    barrier = pltpu.get_barrier_semaphore()

    def greet(**where):
        pl.semaphore_signal(barrier, inc=1, device_id=where)

    loop(ep_count - 1, lambda turn: greet(ep=ep_at(turn)))
    loop(tp_count - 1, lambda turn: greet(tp=tp_at(turn)))

    def room_of(index):
        return pl.ds(pl.multiple_of(index * room, 8), room)

    def feature_lanes(index):
        return pl.ds(pl.multiple_of(index * features, LANES), features)

    model_rows = input_ref[...].astype(jnp.float32)
    scale = lax.rsqrt(jnp.mean(model_rows * model_rows, axis=1, keepdims=True) + norm_eps)
    normed_ref[...] = (model_rows * scale * gain_ref[...]).astype(jnp.bfloat16)

    expert_id = lax.broadcasted_iota(jnp.int32, (LANES, tokens), 0)
    named = jnp.zeros((LANES, tokens), jnp.float32)
    weight_of = jnp.zeros((LANES, tokens), jnp.float32)
    for j in range(routes_ref.shape[0]):
        match = routes_ref[j : j + 1, :] == expert_id
        named = jnp.where(match, 1.0, named)
        weight_of = jnp.where(match, weight_ref[j : j + 1, :], weight_of)
    before = lax.broadcasted_iota(jnp.int32, (tokens, tokens), 0)
    after = lax.broadcasted_iota(jnp.int32, (tokens, tokens), 1)
    earlier = jnp.where(before < after, 1.0, 0.0).astype(jnp.bfloat16)
    ranks = jnp.where(named > 0.0, dot(named.astype(jnp.bfloat16), earlier), -1.0)
    rank_rows[...] = ranks
    weight_rows[...] = weight_of

    piece_lanes = pl.ds(pl.multiple_of(x_me * features + y_me * LANES, LANES), LANES)
    line = lax.broadcasted_iota(jnp.int32, (LANES, tokens), 0)
    marker = jnp.where(line == 0, 1.0, 0.0).astype(jnp.bfloat16)
    marked = jnp.concatenate([ranks.astype(jnp.bfloat16), marker], axis=0)
    own_piece = normed_ref[:, piece_lanes]
    for start in range(0, slot_count, slot_tile):
        span = slice(start, start + slot_tile)
        match = dot(places_ref[span, :], marked)
        pick = jnp.where(match == 0.0, 1.0, 0.0).astype(jnp.bfloat16)
        picked[span, :] = dot(pick, own_piece).astype(jnp.bfloat16)

    q_ref[...] = (query_ref[...].astype(jnp.float32) * HEAD**-0.5).astype(jnp.bfloat16)
    lines = jnp.concatenate([key_ref[:, 0:half], key_ref[:, half:rows]], axis=0)
    kv_ref[0:half, :] = lines.astype(jnp.float32).T.astype(jnp.bfloat16)
    for i in range(chunks):
        kv_ref[half + HEAD * i : half + HEAD * (i + 1), :] = value_ref[:, LANES * i : LANES * (i + 1)]

    minus = -gate_ref[...].T
    high = minus.astype(jnp.bfloat16)
    rest = minus - high.astype(jnp.float32)
    middle = rest.astype(jnp.bfloat16)
    low = (rest - middle.astype(jnp.float32)).astype(jnp.bfloat16)
    gate_rows = gate_ref.shape[0]
    lane = lax.broadcasted_iota(jnp.int32, (gate_rows, LANES), 1)
    shift = lax.broadcasted_iota(jnp.int32, (gate_rows, LANES), 0) - (lane // TERMS) * chunks
    for i in range(chunks):
        terms = jnp.zeros((LANES, LANES), jnp.float32)
        for index, part in enumerate((high, middle, low)):
            spot = jnp.logical_and(shift == i, lane % TERMS == index)
            terms = terms + dot(part, jnp.where(spot, 1.0, 0.0).astype(jnp.bfloat16))
        terms_ref[LANES * i : LANES * (i + 1), :] = terms.astype(jnp.bfloat16)

    acc[...] = jnp.zeros_like(acc)
    row_max[...] = jnp.full_like(row_max, neg_fill)

    pl.semaphore_wait(barrier, ep_count + tp_count - 2)

    def pick_copy(target, owner):
        return pltpu.make_async_remote_copy(
            src_ref=picked.at[room_of(target)],
            dst_ref=pieces.at[y_me, room_of(owner)],
            send_sem=pick_send.at[target],
            recv_sem=pick_recv.at[owner],
            device_id={"ep": target},
        )

    sources = (
        (gate_w.at[:, :, feature_lanes(x_me)], lambda owner: weights.at[0, :, owner]),
        (up_w.at[:, :, feature_lanes(x_me)], lambda owner: weights.at[1, :, owner]),
        (down_w, lambda owner: down_all.at[owner]),
    )

    def weight_copy(index, target, owner):
        source = down_w
        if index < 2:
            source = (gate_w, up_w)[index].at[:, :, feature_lanes(target)]
        return pltpu.make_async_remote_copy(
            src_ref=source,
            dst_ref=sources[index][1](owner),
            send_sem=weight_send.at[index, target],
            recv_sem=weight_recv.at[index, owner],
            device_id={"tp": y_me * wide + target},
        )

    def own_weight(index):
        return pltpu.make_async_copy(
            sources[index][0], sources[index][1](x_me), own_sem.at[index]
        )

    def up_copy(src, slot):
        return pltpu.make_async_remote_copy(
            src_ref=src,
            dst_ref=held.at[slot],
            send_sem=up_send.at[slot],
            recv_sem=kv_recv.at[slot],
            device_id={"ep": me + CORES},
        )

    def down_copy(src, slot):
        return pltpu.make_async_remote_copy(
            src_ref=src,
            dst_ref=held.at[slot],
            send_sem=down_send.at[slot],
            recv_sem=kv_recv.at[slot],
            device_id={"ep": lax.rem(chip + chips - 1, chips) * CORES + core},
        )

    def side_copy(src, slot):
        return pltpu.make_async_remote_copy(
            src_ref=src,
            dst_ref=held.at[slot],
            send_sem=side_send.at[slot],
            recv_sem=kv_recv.at[slot],
            device_id={"ep": chip * CORES + other},
        )

    def piece_copy(group, target, owner):
        place = pieces.at[owner, pl.ds(pl.multiple_of(group * share_rows, 8), share_rows)]
        return pltpu.make_async_remote_copy(
            src_ref=place,
            dst_ref=place,
            send_sem=piece_send.at[target, group],
            recv_sem=piece_recv.at[owner, group],
            device_id={"tp": target * wide + x_me},
        )

    def part_copy(target, owner):
        return pltpu.make_async_remote_copy(
            src_ref=part_out.at[pl.ds(pl.multiple_of(target * share_rows, 8), share_rows)],
            dst_ref=part_in.at[owner],
            send_sem=part_send.at[target],
            recv_sem=part_recv.at[owner],
            device_id={"tp": y_me * wide + target},
        )

    def hidden_copy(target, owner):
        return pltpu.make_async_remote_copy(
            src_ref=hidden_all.at[owner],
            dst_ref=hidden_all.at[owner],
            send_sem=hidden_send.at[target],
            recv_sem=hidden_recv.at[owner],
            device_id={"tp": target * wide + x_me},
        )

    def shared_copy(target, owner):
        return pltpu.make_async_remote_copy(
            src_ref=shared_out,
            dst_ref=shared_all.at[owner],
            send_sem=shared_send.at[target],
            recv_sem=shared_recv.at[owner],
            device_id={"tp": target},
        )

    def share_of(index):
        return pl.ds(pl.multiple_of(index * share_rows, 8), share_rows)

    def cross_copy(target, owner):
        return pltpu.make_async_remote_copy(
            src_ref=result_out.at[target],
            dst_ref=result_all.at[share_of(owner)],
            send_sem=cross_send.at[target],
            recv_sem=cross_recv.at[owner],
            device_id={"tp": y_me * wide + target},
        )

    def own_cross():
        return pltpu.make_async_copy(
            result_out.at[x_me], result_all.at[share_of(x_me)], own_sem.at[5]
        )

    def result_copy(target, owner):
        return pltpu.make_async_remote_copy(
            src_ref=result_all.at[room_of(target)],
            dst_ref=result_in.at[room_of(owner)],
            send_sem=result_send.at[target],
            recv_sem=result_recv.at[owner],
            device_id={"ep": target},
        )

    def own_result():
        return pltpu.make_async_copy(
            result_all.at[room_of(me)], result_in.at[room_of(me)], own_sem.at[4]
        )

    half_head = HEAD // 2

    def row_copy(owner_y, owner_x, part, target, sem):
        place = heads_all.at[owner_y, owner_x, part * half_head : (part + 1) * half_head]
        return pltpu.make_async_remote_copy(
            src_ref=place,
            dst_ref=place,
            send_sem=sem,
            recv_sem=head_recv.at[part, owner_y * wide + owner_x],
            device_id={"tp": y_me * wide + target},
        )

    def column_copy(owner_y, owner_x, part, target, sem):
        place = heads_all.at[owner_y, owner_x, part * half_head : (part + 1) * half_head]
        return pltpu.make_async_remote_copy(
            src_ref=place,
            dst_ref=place,
            send_sem=sem,
            recv_sem=head_recv.at[part, owner_y * wide + owner_x],
            device_id={"tp": target * wide + x_me},
        )

    def row_part(owner_x, target):
        return column_copy(y_me, owner_x, 0, target, column_send.at[0, owner_x, target])

    def row_first(target, owner_x):
        return row_copy(y_me, owner_x, 0, target, row_send.at[1, tall, target])

    def column_part(owner_y, target):
        return row_copy(owner_y, x_me, 1, target, row_send.at[0, owner_y, target])

    def column_first(target, owner_y):
        return column_copy(owner_y, x_me, 1, target, column_send.at[1, wide, target])

    def own_pick():
        return pltpu.make_async_copy(
            picked.at[room_of(me)], pieces.at[y_me, room_of(me)], own_sem.at[3]
        )

    @pl.when(chip < chips - 1)
    def _():
        up_copy(kv_ref, me).start()

    @pl.when(chip <= last_down)
    def _():
        down_copy(kv_ref, me).start()

    @pl.when(core == 0)
    def _():
        side_copy(kv_ref, me).start()

    loop(ep_count - 1, lambda turn: pick_copy(ep_at(turn), me).start())
    own_pick().start()

    loop(wide - 1, lambda turn: weight_copy(0, x_at(turn), x_me).start())
    loop(wide - 1, lambda turn: weight_copy(1, x_at(turn), x_me).start())
    for index in range(3):
        own_weight(index).start()
    loop(wide - 1, lambda turn: weight_copy(2, x_at(turn), x_me).start())

    ones = jnp.ones((acc.shape[0] - HEAD, rows), jnp.bfloat16)
    nothing = jnp.zeros((HEAD, tile), jnp.bfloat16)

    def block_step(block, source, masked):
        mark = lax.broadcasted_iota(jnp.int32, (LANES, tile), 0)
        wanted = jnp.logical_and(mark // TERMS == block, mark % TERMS < TERMS - 1)
        chosen = jnp.where(wanted, 1.0, 0.0).astype(jnp.bfloat16)
        keys = source[0:half, :]
        early = jnp.concatenate([keys, terms_ref[0:half, :]], axis=1)
        late = jnp.concatenate([keys, terms_ref[half:rows, :]], axis=1)
        values = jnp.concatenate(
            [source[half + HEAD * i : half + HEAD * (i + 1), :] for i in range(chunks)], axis=1
        )
        values = jnp.concatenate([values, ones], axis=0)

        def score(start):
            query = q_ref[:, start : start + tile]
            first = dot(early, jnp.concatenate([query, nothing, chosen], axis=0))
            second = dot(late, jnp.concatenate([nothing, query, chosen], axis=0))
            if masked:
                q_pos = start + lax.broadcasted_iota(jnp.int32, first.shape, 1)
                k_pos = lax.broadcasted_iota(jnp.int32, first.shape, 0)
                first = jnp.where(k_pos <= q_pos, first, neg_fill)
                second = jnp.where(k_pos + half <= q_pos, second, neg_fill)
            return first, second

        def soften(start, first, second):
            old_max = row_max[0:1, start : start + tile]
            top = jnp.maximum(
                jnp.max(first, axis=0, keepdims=True), jnp.max(second, axis=0, keepdims=True)
            )
            new_max = jnp.maximum(old_max, top)
            probs = jnp.concatenate(
                [
                    jnp.exp2((first - new_max) * LOG2E).astype(jnp.bfloat16),
                    jnp.exp2((second - new_max) * LOG2E).astype(jnp.bfloat16),
                ],
                axis=0,
            )
            row_max[0:1, start : start + tile] = new_max
            return probs, jnp.exp2((old_max - new_max) * LOG2E)

        def collect(start, probs, keep):
            span = slice(start, start + tile)
            acc[:, span] = acc[:, span] * keep + dot(values, probs)

        starts = list(range(0, rows, tile))
        scores = score(starts[0])
        waiting = None
        for index, start in enumerate(starts):
            upcoming = score(starts[index + 1]) if index + 1 < len(starts) else None
            ready = soften(start, *scores)
            if waiting is not None:
                collect(starts[index - 1], *waiting)
            waiting, scores = ready, upcoming
        collect(starts[-1], *waiting)

    block_step(me, kv_ref, True)

    def local_stage():
        column = lax.broadcasted_iota(jnp.int32, (tokens, LANES), 1)
        marker = jnp.where(column == 0, 1.0, 0.0).astype(jnp.bfloat16)
        marked = jnp.concatenate([rank_rows[...].T.astype(jnp.bfloat16), marker], axis=1)
        weight = weight_rows[...].T
        high = weight.astype(jnp.bfloat16)
        low = (weight - high.astype(jnp.float32)).astype(jnp.bfloat16)
        for start in range(0, slot_count, slot_tile):
            span = slice(start, start + slot_tile)
            match = dot_nt(marked, places_ref[span, :])
            for index, part in enumerate((high, low)):
                value = dot_nt(part, places_ref[span, 0:LANES])
                spread[index, :, span] = jnp.where(match == 0.0, value, 0.0).astype(jnp.bfloat16)
        shared = silu(dot_nt(shared_gate_ref[...], normed_ref[...])) * dot_nt(
            shared_up_ref[...], normed_ref[...]
        )
        shared_out[...] = jnp.zeros_like(shared_out)
        shared_out[:, 0:tokens] = shared.astype(jnp.bfloat16)
        shared_all[tp_me] = shared_out[...]
        loop(tp_count - 1, lambda turn: shared_copy(tp_at(turn), tp_me).start())
        mix_weight[...] = out_weight_ref[...].astype(jnp.float32).T.astype(jnp.bfloat16)
        shared_weight[...] = shared_down_ref[...].astype(jnp.float32).T.astype(jnp.bfloat16)

    def choose(parts):
        owner = owner_ref[:, 0:1]
        value = parts[0]
        for index in range(1, experts):
            value = jnp.where(owner == float(index), parts[index], value)
        return value

    def forward_group(group):
        def wait_block(turn):
            source = group * share + turn

            @pl.when(source != me)
            def _():
                pick_copy(source, source).wait_recv()

        loop(share, wait_block)
        loop(tall - 1, lambda turn: piece_copy(group, y_at(turn), y_me).start())

    def near_stage():
        own_pick().wait()
        forward_group(keeper)

    def far_stage():
        loop(wide, lambda turn: forward_group(lax.rem(keeper + turn, wide)), 1)

    def parts_stage():
        def wait_pieces(group):
            loop(tall - 1, lambda turn: piece_copy(group, y_at(turn), y_at(turn)).wait_recv())

        loop(wide, wait_pieces)
        for index in range(2):
            loop(wide - 1, lambda turn: weight_copy(index, x_at(turn), x_at(turn)).wait_recv())
            own_weight(index).wait()

        def one_tile(index):
            span = share_of(index)
            rows_of = jnp.concatenate([pieces[y, span, :] for y in range(tall)], axis=1)
            parts = []
            for e in range(experts):
                block = jnp.concatenate(
                    [weights[g, e].reshape(wide * own_hidden, features) for g in range(2)], axis=0
                )
                parts.append(dot_nt(rows_of, block))
            part_out[span, :] = choose(parts).astype(jnp.bfloat16)

        loop(wide, one_tile)
        loop(wide - 1, lambda turn: part_copy(x_at(turn), x_me).start())

    def hidden_stage():
        loop(wide - 1, lambda turn: part_copy(x_at(turn), x_at(turn)).wait_recv())
        own_rows = pl.ds(pl.multiple_of(x_me * share_rows, 8), share_rows)
        total = part_out[own_rows, :].astype(jnp.float32)
        for turn in range(wide - 1):
            total = total + part_in[x_at(turn)].astype(jnp.float32)
        middle = wide * own_hidden
        hidden = silu(total[:, 0:middle]) * total[:, middle:]
        hidden_all[y_me] = hidden.astype(jnp.bfloat16)
        loop(tall - 1, lambda turn: hidden_copy(y_at(turn), y_me).start())

    def down_stage():
        loop(tall - 1, lambda turn: hidden_copy(y_at(turn), y_at(turn)).wait_recv())
        loop(wide - 1, lambda turn: weight_copy(2, x_at(turn), x_at(turn)).wait_recv())
        own_weight(2).wait()
        units = jnp.concatenate([hidden_all[y] for y in range(tall)], axis=1)
        for x in range(0, wide, 2):
            results = [
                dot(units, jnp.concatenate([down_all[x, e], down_all[x + 1, e]], axis=1))
                for e in range(experts)
            ]
            result = choose(results).astype(jnp.bfloat16)
            columns = result.shape[1] // 2
            result_out[x] = result[:, 0:columns]
            result_out[x + 1] = result[:, columns:]

        loop(wide - 1, lambda turn: cross_copy(x_at(turn), x_me).start())
        own_cross().start()

    def return_stage():
        loop(wide - 1, lambda turn: cross_copy(x_at(turn), x_at(turn)).wait_recv())
        own_cross().wait()
        loop(ep_count - 1, lambda turn: result_copy(ep_at(turn), me).start())
        own_result().start()

    def received(hop, downward):
        going_up = jnp.logical_and(hop >= 1, jnp.logical_and(hop <= up_hops, chip - hop >= 0))
        source = lax.rem(chip + hop, chips)
        going_down = jnp.logical_and(
            hop >= 1, jnp.logical_and(hop <= down_hops, source <= last_down)
        )
        return jnp.where(downward, going_down, going_up)

    def useful(hop, downward):
        return jnp.logical_and(
            received(hop, downward), jnp.logical_or(jnp.logical_not(downward), chip + hop >= chips)
        )

    def forwards_up(hop):
        return jnp.logical_and(
            received(hop, False), jnp.logical_and(hop < up_hops, chip < chips - 1)
        )

    def forwards_down(hop):
        return jnp.logical_and(received(hop, True), hop < down_hops)

    def home_of(hop, downward):
        return jnp.where(downward, lax.rem(chip + hop, chips), chip - hop)

    def carry_on(hop, downward):
        slot = home_of(hop, downward) * CORES + core

        @pl.when(received(hop, downward))
        def _():
            up_copy(held.at[slot], slot).wait_recv()

        @pl.when(jnp.logical_and(jnp.logical_not(downward), forwards_up(hop)))
        def _():
            up_copy(held.at[slot], slot).start()

        @pl.when(jnp.logical_and(downward, forwards_down(hop)))
        def _():
            down_copy(held.at[slot], slot).start()

        @pl.when(useful(hop, downward))
        def _():
            side_copy(held.at[slot], slot).start()

    def substep(index):
        pl.when(jnp.logical_and(index >= 4, index % 3 != 0))(
            lambda: carry_on((index - 1) // 3, index % 3 == 2)
        )
        hop = index // 4
        kind = index % 4
        downward = kind % 2 == 1
        own_core = kind < 2
        slot = home_of(hop, downward) * CORES + jnp.where(own_core, core, other)
        sibling = jnp.logical_and(index == 2, core == 1)
        used = useful(hop, downward)

        @pl.when(jnp.logical_or(jnp.logical_and(jnp.logical_not(own_core), used), sibling))
        def _():
            side_copy(held.at[slot], slot).wait_recv()

        @pl.when(jnp.logical_or(used, sibling))
        def _():
            block_step(slot, held.at[slot], False)

        pl.when(index == LOCAL_AT)(local_stage)
        pl.when(index == NEAR_AT)(near_stage)
        pl.when(index == FAR_AT)(far_stage)
        pl.when(index == PARTS_AT)(parts_stage)
        pl.when(index == HIDDEN_AT)(hidden_stage)
        pl.when(index == DOWN_AT)(down_stage)
        pl.when(index == RETURN_AT)(return_stage)

    loop(max(4 * up_hops + 4, RETURN_AT + 1), substep, 2)

    heads = acc[0:HEAD] / acc[HEAD : HEAD + 1]
    heads_all[y_me, x_me] = heads.astype(jnp.bfloat16)
    loop(wide - 1, lambda turn: row_first(x_at(turn), x_me).start())
    loop(tall - 1, lambda turn: column_first(y_at(turn), y_me).start())
    loop(tall - 1, lambda turn: row_part(x_me, y_at(turn)).start())
    loop(wide - 1, lambda turn: column_part(y_me, x_at(turn)).start())

    def pass_row(turn):
        row_first(x_at(turn), x_at(turn)).wait_recv()
        loop(tall - 1, lambda way: row_part(x_at(turn), y_at(way)).start())

    def pass_column(turn):
        column_first(y_at(turn), y_at(turn)).wait_recv()
        loop(wide - 1, lambda way: column_part(y_at(turn), x_at(way)).start())

    loop(wide - 1, pass_row)
    loop(tall - 1, pass_column)

    loop(ep_count - 1, lambda turn: result_copy(ep_at(turn), ep_at(turn)).wait_recv())
    own_result().wait()
    loop(tp_count - 1, lambda turn: shared_copy(tp_at(turn), tp_at(turn)).wait_recv())
    shared_units = shared_all[...].reshape(tp_count * own_hidden, -1)
    shared_sum = dot(shared_weight[...], shared_units).T[0:tokens]
    routed = dot(spread[0], result_in[...]) + dot(spread[1], result_in[...])
    moe_ref[...] = (routed + shared_sum).astype(moe_ref.dtype)

    def finish_ep(turn):
        pick_copy(ep_at(turn), me).wait_send()
        result_copy(ep_at(turn), me).wait_send()

    loop(ep_count - 1, finish_ep)

    def finish_pieces(group):
        loop(tall - 1, lambda turn: piece_copy(group, y_at(turn), y_me).wait_send())

    loop(wide, finish_pieces)

    def finish_x(turn):
        for index in range(3):
            weight_copy(index, x_at(turn), x_me).wait_send()
        part_copy(x_at(turn), x_me).wait_send()
        cross_copy(x_at(turn), x_me).wait_send()

    loop(wide - 1, finish_x)
    loop(tall - 1, lambda turn: hidden_copy(y_at(turn), y_me).wait_send())
    loop(tp_count - 1, lambda turn: shared_copy(tp_at(turn), tp_me).wait_send())

    @pl.when(chip < chips - 1)
    def _():
        up_copy(kv_ref, me).wait_send()

    @pl.when(chip <= last_down)
    def _():
        down_copy(kv_ref, me).wait_send()

    @pl.when(core == 0)
    def _():
        side_copy(kv_ref, me).wait_send()

    def finish_hop(hop):
        low_slot = home_of(hop, False) * CORES + core
        high_slot = home_of(hop, True) * CORES + core

        @pl.when(forwards_up(hop))
        def _():
            up_copy(held.at[low_slot], low_slot).wait_send()

        @pl.when(forwards_down(hop))
        def _():
            down_copy(held.at[high_slot], high_slot).wait_send()

        @pl.when(useful(hop, False))
        def _():
            side_copy(held.at[low_slot], low_slot).wait_send()

        @pl.when(useful(hop, True))
        def _():
            side_copy(held.at[high_slot], high_slot).wait_send()

    loop(up_hops + 1, finish_hop, 1)

    def wait_far(turn):
        y = y_at(turn)

        def one(way):
            x = lax.rem(x_me + way, wide)
            column_copy(y, x, 0, 0, column_send.at[0, 0, 0]).wait_recv()

        loop(wide, one)

    def wait_wide(turn):
        x = x_at(turn)

        def one(way):
            y = lax.rem(y_me + way, tall)
            row_copy(y, x, 1, 0, row_send.at[0, 0, 0]).wait_recv()

        loop(tall, one)

    loop(tall - 1, wait_far)
    loop(wide - 1, wait_wide)
    for start in range(0, rows, tile):
        span = slice(start, start + tile)
        units = heads_all[:, :, :, span].reshape(tp_count * HEAD, tile)
        mixed = dot(mix_weight[...], units)
        mixer_ref[span, :] = mixed.T.astype(mixer_ref.dtype)

    def finish_row(turn):
        row_first(x_at(turn), x_me).wait_send()
        loop(tall, lambda y: column_part(y, x_at(turn)).wait_send())

    def finish_column(turn):
        column_first(y_at(turn), y_me).wait_send()
        loop(wide, lambda x: row_part(x, y_at(turn)).wait_send())

    loop(wide - 1, finish_row)
    loop(tall - 1, finish_column)


def slot_tables(ep_count, wide, experts, cap, room):
    slot = np.arange(ep_count * room)
    inside = slot % room
    real = inside < experts * cap
    places = np.zeros((slot.size, 2 * LANES), np.float32)
    expert = (slot // room) * experts + inside // cap
    places[slot[real], expert[real]] = 1.0
    places[:, LANES] = np.where(real, -(inside % cap), 5.0)
    owner = np.where(real, inside // cap, 0).astype(np.float32)
    owner = np.tile(owner[: slot.size // wide, None], (1, LANES))
    return jnp.asarray(places, jnp.bfloat16), jnp.asarray(owner, jnp.float32)


def local(
    query_rows,
    key_rows,
    value_rows,
    cum_gate,
    out_weight,
    moe_input,
    moe_gain,
    routes,
    route_weight,
    expert_gate,
    expert_up,
    expert_down,
    shared_gate,
    shared_up,
    shared_down,
):
    rows, width = query_rows.shape
    token_count = moe_input.shape[0]
    top_count = routes.shape[1]
    experts, model, own_hidden = expert_gate.shape
    ep_count = lax.axis_size("ep")
    tp_count = lax.axis_size("tp")
    wide, tall = plane_shape(tp_count)
    expert_count = experts * ep_count
    cap = 2 * token_count * top_count // expert_count
    room = -(-experts * cap // 8) * 8
    slot_count = ep_count * room
    share_rows = slot_count // wide
    token_span = -(-token_count // LANES) * LANES
    columns = expert_down.shape[2]

    places, owner = slot_tables(ep_count, wide, experts, cap, room)
    dma = pltpu.SemaphoreType.DMA
    vmem = pl.BlockSpec(memory_space=pltpu.VMEM)
    anywhere = pl.BlockSpec(memory_space=pl.ANY)
    blocks = ep_count * rows * rows
    bf16 = jnp.bfloat16
    mixer_out, moe_out = pl.pallas_call(
        functools.partial(layer_kernel, cap, room),
        out_shape=[
            jax.ShapeDtypeStruct((rows, columns), bf16),
            jax.ShapeDtypeStruct((token_count, columns), bf16),
        ],
        in_specs=[vmem] * 10 + [anywhere] * 3 + [vmem] * 4,
        out_specs=[vmem, vmem],
        scratch_shapes=[
            pltpu.VMEM((HEAD, rows), bf16),
            pltpu.VMEM((rows, LANES), bf16),
            pltpu.VMEM((rows, LANES), bf16),
            pltpu.VMEM((token_count, model), bf16),
            pltpu.VMEM((LANES, token_count), jnp.float32),
            pltpu.VMEM((LANES, token_count), jnp.float32),
            pltpu.VMEM((columns, tp_count * HEAD), bf16),
            pltpu.VMEM((columns, tp_count * own_hidden), bf16),
            pltpu.VMEM((ep_count, rows, LANES), bf16),
            pltpu.VMEM((HEAD + 16, rows), jnp.float32),
            pltpu.VMEM((8, rows), jnp.float32),
            pltpu.VMEM((slot_count, LANES), bf16),
            pltpu.VMEM((tall, slot_count, LANES), bf16),
            pltpu.VMEM((2, experts, wide, own_hidden, model // wide), bf16),
            pltpu.VMEM((wide, experts, tp_count * own_hidden, columns), bf16),
            pltpu.VMEM((slot_count, 2 * wide * own_hidden), bf16),
            pltpu.VMEM((wide, share_rows, 2 * wide * own_hidden), bf16),
            pltpu.VMEM((tall, share_rows, wide * own_hidden), bf16),
            pltpu.VMEM((own_hidden, token_span), bf16),
            pltpu.VMEM((tp_count, own_hidden, token_span), bf16),
            pltpu.VMEM((wide, share_rows, columns), bf16),
            pltpu.VMEM((slot_count, columns), bf16),
            pltpu.VMEM((slot_count, columns), bf16),
            pltpu.VMEM((2, token_count, slot_count), bf16),
            pltpu.VMEM((tall, wide, HEAD, rows), bf16),
        ]
        + [dma((ep_count,))] * 8
        + [dma((wide,))] * 2
        + [dma((tall, wide))] * 2
        + [dma((3, wide))] * 2
        + [dma((wide,))] * 2
        + [dma((tall,))] * 2
        + [dma((tp_count,))] * 2
        + [dma((2, tall + 1, wide)), dma((2, wide + 1, tall)), dma((2, tp_count))]
        + [dma((6,))],
        compiler_params=pltpu.CompilerParams(
            collective_id=0, has_side_effects=True, vmem_limit_bytes=56 * 1024 * 1024
        ),
        cost_estimate=pl.CostEstimate(
            flops=blocks * 2 * 512, bytes_accessed=8 * 1024 * 1024, transcendentals=blocks
        ),
        name="layer",
    )(
        query_rows.T,
        key_rows.T,
        value_rows.T,
        cum_gate.reshape(-1, LANES),
        moe_input,
        moe_gain.reshape(1, -1),
        routes.T,
        route_weight.T,
        places,
        owner,
        expert_gate.transpose(0, 2, 1),
        expert_up.transpose(0, 2, 1),
        expert_down,
        shared_gate.T,
        shared_up.T,
        shared_down,
        out_weight,
    )
    return mixer_out, moe_out


def solution(mesh):
    placed = (
        P("ep", "tp"),
        P("ep", "tp"),
        P("ep", "tp"),
        P("tp", None),
        P(None, "tp"),
        P("ep", None),
        P(),
        P("ep", None),
        P("ep", None),
        P("ep", None, "tp"),
        P("ep", None, "tp"),
        P("ep", None, "tp"),
        P(None, "tp"),
        P(None, "tp"),
        P(None, "tp"),
    )
    return jax.shard_map(
        local, mesh=mesh, in_specs=placed, out_specs=(P("ep", "tp"), P("ep", "tp")), check_vma=False
    )
```

```python
import functools

import jax
import jax.numpy as jnp
import numpy as np
from jax import lax
from jax.experimental import pallas as pl
from jax.experimental.pallas import tpu as pltpu
from jax.sharding import PartitionSpec as P

HEAD = 64
LANES = 128
CORES = 2
TERMS = 4
LOG2E = 1.4426950408889634

neg_fill = -1e30
norm_eps = 1e-06

LOCAL_AT = 5
GATHER_AT = (7, 10)
PARTS_AT = (9, 16)
HIDDEN_AT = (12, 20)
DOWN_AT = (19, 24)
RETURN_AT = (23, 28)


def plane_shape(tp_count):
    wide = 1
    while wide * wide < tp_count:
        wide *= 2
    return wide, tp_count // wide


def dot(a, b):
    return jnp.dot(a, b, preferred_element_type=jnp.float32)


def dot_nt(a, b):
    return lax.dot_general(a, b, (((1,), (1,)), ((), ())), preferred_element_type=jnp.float32)


def silu(v):
    return v / (1.0 + jnp.exp(-v))


def loop(count, body, first=0):
    def step(index, carry):
        body(index)
        return carry

    lax.fori_loop(first, count, step, 0)


def layer_kernel(
    cap,
    room,
    query_ref,
    key_ref,
    value_ref,
    gate_ref,
    input_ref,
    gain_ref,
    routes_ref,
    weight_ref,
    places_ref,
    owner_ref,
    gate_w,
    up_w,
    down_w,
    shared_gate_ref,
    shared_up_ref,
    shared_down_ref,
    out_weight_ref,
    mixer_ref,
    moe_ref,
    q_ref,
    kv_ref,
    terms_ref,
    normed_ref,
    weight_rows,
    rank_rows,
    mix_weight,
    shared_weight,
    held,
    acc,
    row_max,
    picked,
    pieces,
    weights,
    down_all,
    part_out,
    part_in,
    hidden_all,
    shared_out,
    shared_all,
    result_out,
    result_all,
    result_in,
    spread,
    heads_all,
    up_send,
    down_send,
    side_send,
    kv_recv,
    pick_send,
    pick_recv,
    result_send,
    result_recv,
    cross_send,
    cross_recv,
    piece_send,
    piece_recv,
    weight_send,
    weight_recv,
    part_send,
    part_recv,
    hidden_send,
    hidden_recv,
    shared_send,
    shared_recv,
    row_send,
    column_send,
    head_recv,
    own_sem,
    own_cross_sem,
):
    rows = q_ref.shape[1]
    half = rows // 2
    chunks = rows // LANES
    tile = 256 if rows % 256 == 0 else rows
    tokens = normed_ref.shape[0]
    experts = gate_w.shape[0]
    own_hidden = gate_w.shape[1]
    slot_count = picked.shape[0]
    slot_tile = 256 if slot_count % 256 == 0 else slot_count

    me = lax.axis_index("ep")
    ep_count = lax.axis_size("ep")
    chips = ep_count // CORES
    chip = me // CORES
    core = me % CORES
    other = 1 - core
    tp_count = lax.axis_size("tp")
    tp_me = lax.axis_index("tp")
    wide, tall = plane_shape(tp_count)
    x_me = tp_me % wide
    y_me = tp_me // wide
    up_hops = chips // 2
    down_hops = chips - 1 - up_hops
    last_down = chips - 2 - up_hops
    features = normed_ref.shape[1] // wide
    share = ep_count // wide
    share_rows = share * room
    half_share = share // 2
    half_rows = half_share * room
    reach = chips // 4

    def place_of(block, home):
        offset = lax.rem(block // CORES - home // CORES + reach + chips, chips)
        rank = lax.rem(offset, chips // 2) * CORES + block % CORES
        far = offset // (chips // 2)
        return rank // half_share * share + far * half_share + lax.rem(rank, half_share)

    def block_at(rank, far):
        offset = rank // CORES + far * (chips // 2)
        return lax.rem(chip - reach + offset + chips, chips) * CORES + rank % CORES

    def target_at(rank, far):
        offset = rank // CORES + far * (chips // 2)
        return lax.rem(chip + reach - offset + chips, chips) * CORES + rank % CORES

    def ep_at(turn):
        return lax.rem(me + turn + 1, ep_count)

    def tp_at(turn):
        return lax.rem(tp_me + turn + 1, tp_count)

    def x_at(turn):
        return lax.rem(x_me + turn + 1, wide)

    def y_at(turn):
        return lax.rem(y_me + turn + 1, tall)

    barrier = pltpu.get_barrier_semaphore()

    def greet(**where):
        pl.semaphore_signal(barrier, inc=1, device_id=where)

    loop(ep_count - 1, lambda turn: greet(ep=ep_at(turn)))
    loop(tp_count - 1, lambda turn: greet(tp=tp_at(turn)))

    def room_of(index):
        return pl.ds(pl.multiple_of(index * room, 8), room)

    def feature_lanes(index):
        return pl.ds(pl.multiple_of(index * features, LANES), features)

    model_rows = input_ref[...].astype(jnp.float32)
    scale = lax.rsqrt(jnp.mean(model_rows * model_rows, axis=1, keepdims=True) + norm_eps)
    normed_ref[...] = (model_rows * scale * gain_ref[...]).astype(jnp.bfloat16)

    expert_id = lax.broadcasted_iota(jnp.int32, (LANES, tokens), 0)
    named = jnp.zeros((LANES, tokens), jnp.float32)
    weight_of = jnp.zeros((LANES, tokens), jnp.float32)
    for j in range(routes_ref.shape[0]):
        match = routes_ref[j : j + 1, :] == expert_id
        named = jnp.where(match, 1.0, named)
        weight_of = jnp.where(match, weight_ref[j : j + 1, :], weight_of)
    before = lax.broadcasted_iota(jnp.int32, (tokens, tokens), 0)
    after = lax.broadcasted_iota(jnp.int32, (tokens, tokens), 1)
    earlier = jnp.where(before < after, 1.0, 0.0).astype(jnp.bfloat16)
    ranks = jnp.where(named > 0.0, dot(named.astype(jnp.bfloat16), earlier), -1.0)
    rank_rows[...] = ranks
    weight_rows[...] = weight_of

    piece_lanes = pl.ds(pl.multiple_of(x_me * features + y_me * LANES, LANES), LANES)
    line = lax.broadcasted_iota(jnp.int32, (LANES, tokens), 0)
    marker = jnp.where(line == 0, 1.0, 0.0).astype(jnp.bfloat16)
    marked = jnp.concatenate([ranks.astype(jnp.bfloat16), marker], axis=0)
    own_piece = normed_ref[:, piece_lanes]
    for start in range(0, slot_count, slot_tile):
        span = slice(start, start + slot_tile)
        match = dot(places_ref[span, :], marked)
        pick = jnp.where(match == 0.0, 1.0, 0.0).astype(jnp.bfloat16)
        picked[span, :] = dot(pick, own_piece).astype(jnp.bfloat16)

    q_ref[...] = (query_ref[...].astype(jnp.float32) * HEAD**-0.5).astype(jnp.bfloat16)
    lines = jnp.concatenate([key_ref[:, 0:half], key_ref[:, half:rows]], axis=0)
    kv_ref[0:half, :] = lines.astype(jnp.float32).T.astype(jnp.bfloat16)
    for i in range(chunks):
        kv_ref[half + HEAD * i : half + HEAD * (i + 1), :] = value_ref[:, LANES * i : LANES * (i + 1)]

    minus = -gate_ref[...].T
    high = minus.astype(jnp.bfloat16)
    rest = minus - high.astype(jnp.float32)
    middle = rest.astype(jnp.bfloat16)
    low = (rest - middle.astype(jnp.float32)).astype(jnp.bfloat16)
    gate_rows = gate_ref.shape[0]
    lane = lax.broadcasted_iota(jnp.int32, (gate_rows, LANES), 1)
    shift = lax.broadcasted_iota(jnp.int32, (gate_rows, LANES), 0) - (lane // TERMS) * chunks
    for i in range(chunks):
        terms = jnp.zeros((LANES, LANES), jnp.float32)
        for index, part in enumerate((high, middle, low)):
            spot = jnp.logical_and(shift == i, lane % TERMS == index)
            terms = terms + dot(part, jnp.where(spot, 1.0, 0.0).astype(jnp.bfloat16))
        terms_ref[LANES * i : LANES * (i + 1), :] = terms.astype(jnp.bfloat16)

    acc[...] = jnp.zeros_like(acc)
    row_max[...] = jnp.full_like(row_max, neg_fill)

    pl.semaphore_wait(barrier, ep_count + tp_count - 2)

    def pick_copy(target, owner):
        return pltpu.make_async_remote_copy(
            src_ref=picked.at[room_of(target)],
            dst_ref=pieces.at[y_me, room_of(place_of(owner, target))],
            send_sem=pick_send.at[target],
            recv_sem=pick_recv.at[owner],
            device_id={"ep": target},
        )

    def weight_ends(index, target, owner):
        if index < 2:
            source = (gate_w, up_w)[index].at[:, :, feature_lanes(target)]
            return source, weights.at[index, :, owner]
        return down_w.at[index - 2], down_all.at[owner, index - 2]

    def weight_copy(index, target, owner):
        source, place = weight_ends(index, target, owner)
        return pltpu.make_async_remote_copy(
            src_ref=source,
            dst_ref=place,
            send_sem=weight_send.at[index, target],
            recv_sem=weight_recv.at[index, owner],
            device_id={"tp": y_me * wide + target},
        )

    def own_weight(index):
        source, place = weight_ends(index, x_me, x_me)
        return pltpu.make_async_copy(source, place, own_sem.at[index])

    weight_count = 2 + experts
    early_weights = 2 + experts // 2

    def send_weight(index):
        loop(wide - 1, lambda turn: weight_copy(index, x_at(turn), x_me).start())

    def kv_copy(part, slot, own, send_sem, place):
        span = pl.ds(part * half, half)
        return pltpu.make_async_remote_copy(
            src_ref=kv_ref.at[span] if own else held.at[slot, span],
            dst_ref=held.at[slot, span],
            send_sem=send_sem.at[part, slot],
            recv_sem=kv_recv.at[part, slot],
            device_id={"ep": place},
        )

    def up_copy(part, slot, own=False):
        return kv_copy(part, slot, own, up_send, me + CORES)

    def down_copy(part, slot, own=False):
        below = lax.rem(chip + chips - 1, chips) * CORES + core
        return kv_copy(part, slot, own, down_send, below)

    def side_copy(part, slot, own=False):
        return kv_copy(part, slot, own, side_send, chip * CORES + other)

    def piece_copy(far, group, target, owner):
        place = pieces.at[owner, rows_at(group, far)]
        return pltpu.make_async_remote_copy(
            src_ref=place,
            dst_ref=place,
            send_sem=piece_send.at[target, far * wide + group],
            recv_sem=piece_recv.at[owner, far * wide + group],
            device_id={"tp": target * wide + x_me},
        )

    def part_copy(far, target, owner):
        return pltpu.make_async_remote_copy(
            src_ref=part_out.at[rows_at(target, far)],
            dst_ref=part_in.at[owner, far],
            send_sem=part_send.at[far, target],
            recv_sem=part_recv.at[far, owner],
            device_id={"tp": y_me * wide + target},
        )

    def hidden_copy(far, target, owner):
        return pltpu.make_async_remote_copy(
            src_ref=hidden_all.at[owner, far],
            dst_ref=hidden_all.at[owner, far],
            send_sem=hidden_send.at[far, target],
            recv_sem=hidden_recv.at[far, owner],
            device_id={"tp": target * wide + x_me},
        )

    def shared_copy(target, owner):
        return pltpu.make_async_remote_copy(
            src_ref=shared_out,
            dst_ref=shared_all.at[owner],
            send_sem=shared_send.at[target],
            recv_sem=shared_recv.at[owner],
            device_id={"tp": target},
        )

    def rows_at(index, far):
        start = index * share_rows + far * half_rows
        return pl.ds(pl.multiple_of(start, 8), half_rows)

    def cross_copy(far, target, owner):
        return pltpu.make_async_remote_copy(
            src_ref=result_out.at[target, far],
            dst_ref=result_all.at[rows_at(owner, far)],
            send_sem=cross_send.at[far, target],
            recv_sem=cross_recv.at[far, owner],
            device_id={"tp": y_me * wide + target},
        )

    def own_cross(far):
        return pltpu.make_async_copy(
            result_out.at[x_me, far], result_all.at[rows_at(x_me, far)], own_cross_sem.at[far]
        )

    def result_copy(target, owner):
        return pltpu.make_async_remote_copy(
            src_ref=result_all.at[room_of(place_of(target, me))],
            dst_ref=result_in.at[room_of(owner)],
            send_sem=result_send.at[target],
            recv_sem=result_recv.at[owner],
            device_id={"ep": target},
        )

    def own_result():
        return pltpu.make_async_copy(
            result_all.at[room_of(place_of(me, me))],
            result_in.at[room_of(me)],
            own_sem.at[weight_count],
        )

    half_head = HEAD // 2

    def row_copy(owner_y, owner_x, part, target, sem):
        place = heads_all.at[owner_y, owner_x, part * half_head : (part + 1) * half_head]
        return pltpu.make_async_remote_copy(
            src_ref=place,
            dst_ref=place,
            send_sem=sem,
            recv_sem=head_recv.at[part, owner_y * wide + owner_x],
            device_id={"tp": y_me * wide + target},
        )

    def column_copy(owner_y, owner_x, part, target, sem):
        place = heads_all.at[owner_y, owner_x, part * half_head : (part + 1) * half_head]
        return pltpu.make_async_remote_copy(
            src_ref=place,
            dst_ref=place,
            send_sem=sem,
            recv_sem=head_recv.at[part, owner_y * wide + owner_x],
            device_id={"tp": target * wide + x_me},
        )

    def row_part(owner_x, target):
        return column_copy(y_me, owner_x, 0, target, column_send.at[0, owner_x, target])

    def row_first(target, owner_x):
        return row_copy(y_me, owner_x, 0, target, row_send.at[1, tall, target])

    def column_part(owner_y, target):
        return row_copy(owner_y, x_me, 1, target, row_send.at[0, owner_y, target])

    def column_first(target, owner_y):
        return column_copy(owner_y, x_me, 1, target, column_send.at[1, wide, target])

    def own_pick():
        return pltpu.make_async_copy(
            picked.at[room_of(me)],
            pieces.at[y_me, room_of(place_of(me, me))],
            own_sem.at[weight_count + 1],
        )

    @pl.when(chip < chips - 1)
    def _():
        for part in range(2):
            up_copy(part, me, True).start()

    @pl.when(chip <= last_down)
    def _():
        for part in range(2):
            down_copy(part, me, True).start()

    @pl.when(core == 0)
    def _():
        for part in range(2):
            side_copy(part, me, True).start()

    def send_picked(far):
        def one(rank):
            target = target_at(rank, far)

            @pl.when(target != me)
            def _():
                pick_copy(target, me).start()

        loop(ep_count // 2, one)

    send_picked(0)
    own_pick().start()
    for index in range(weight_count):
        own_weight(index).start()
    for index in range(early_weights):
        send_weight(index)

    ones = jnp.ones((acc.shape[0] - HEAD, rows), jnp.bfloat16)
    nothing = jnp.zeros((HEAD, tile), jnp.bfloat16)

    def block_step(block, source, masked):
        mark = lax.broadcasted_iota(jnp.int32, (LANES, tile), 0)
        wanted = jnp.logical_and(mark // TERMS == block, mark % TERMS < TERMS - 1)
        chosen = jnp.where(wanted, 1.0, 0.0).astype(jnp.bfloat16)
        keys = source[0:half, :]
        early = jnp.concatenate([keys, terms_ref[0:half, :]], axis=1)
        late = jnp.concatenate([keys, terms_ref[half:rows, :]], axis=1)
        values = jnp.concatenate(
            [source[half + HEAD * i : half + HEAD * (i + 1), :] for i in range(chunks)], axis=1
        )
        values = jnp.concatenate([values, ones], axis=0)

        def score(start):
            query = q_ref[:, start : start + tile]
            first = dot(early, jnp.concatenate([query, nothing, chosen], axis=0))
            second = dot(late, jnp.concatenate([nothing, query, chosen], axis=0))
            if masked:
                q_pos = start + lax.broadcasted_iota(jnp.int32, first.shape, 1)
                k_pos = lax.broadcasted_iota(jnp.int32, first.shape, 0)
                first = jnp.where(k_pos <= q_pos, first, neg_fill)
                second = jnp.where(k_pos + half <= q_pos, second, neg_fill)
            return first, second

        def soften(start, first, second):
            old_max = row_max[0:1, start : start + tile]
            top = jnp.maximum(
                jnp.max(first, axis=0, keepdims=True), jnp.max(second, axis=0, keepdims=True)
            )
            new_max = jnp.maximum(old_max, top)
            probs = jnp.concatenate(
                [
                    jnp.exp2((first - new_max) * LOG2E).astype(jnp.bfloat16),
                    jnp.exp2((second - new_max) * LOG2E).astype(jnp.bfloat16),
                ],
                axis=0,
            )
            row_max[0:1, start : start + tile] = new_max
            return probs, jnp.exp2((old_max - new_max) * LOG2E)

        def collect(start, probs, keep):
            span = slice(start, start + tile)
            acc[:, span] = acc[:, span] * keep + dot(values, probs)

        starts = list(range(0, rows, tile))
        scores = score(starts[0])
        waiting = None
        for index, start in enumerate(starts):
            upcoming = score(starts[index + 1]) if index + 1 < len(starts) else None
            ready = soften(start, *scores)
            if waiting is not None:
                collect(starts[index - 1], *waiting)
            waiting, scores = ready, upcoming
        collect(starts[-1], *waiting)

    block_step(me, kv_ref, True)

    def local_stage():
        send_picked(1)

        column = lax.broadcasted_iota(jnp.int32, (tokens, LANES), 1)
        marker = jnp.where(column == 0, 1.0, 0.0).astype(jnp.bfloat16)
        marked = jnp.concatenate([rank_rows[...].T.astype(jnp.bfloat16), marker], axis=1)
        weight = weight_rows[...].T
        high = weight.astype(jnp.bfloat16)
        low = (weight - high.astype(jnp.float32)).astype(jnp.bfloat16)
        for start in range(0, slot_count, slot_tile):
            span = slice(start, start + slot_tile)
            match = dot_nt(marked, places_ref[span, :])
            for index, part in enumerate((high, low)):
                value = dot_nt(part, places_ref[span, 0:LANES])
                spread[index, :, span] = jnp.where(match == 0.0, value, 0.0).astype(jnp.bfloat16)
        shared = silu(dot_nt(shared_gate_ref[...], normed_ref[...])) * dot_nt(
            shared_up_ref[...], normed_ref[...]
        )
        shared_out[...] = jnp.zeros_like(shared_out)
        shared_out[:, 0:tokens] = shared.astype(jnp.bfloat16)
        shared_all[tp_me] = shared_out[...]
        loop(tp_count - 1, lambda turn: shared_copy(tp_at(turn), tp_me).start())
        mix_weight[...] = out_weight_ref[...].astype(jnp.float32).T.astype(jnp.bfloat16)
        shared_weight[...] = shared_down_ref[...].astype(jnp.float32).T.astype(jnp.bfloat16)

    def choose(parts):
        owner = owner_ref[0 : parts[0].shape[0], 0:1]
        value = parts[0]
        for index in range(1, experts):
            value = jnp.where(owner == float(index), parts[index], value)
        return value

    def gather_stage(far):
        @pl.when(far == 0)
        def _():
            own_pick().wait()

        def one_group(group):
            def wait_block(turn):
                source = block_at(group * half_share + turn, far)

                @pl.when(source != me)
                def _():
                    pick_copy(source, source).wait_recv()

            loop(half_share, wait_block)
            loop(tall - 1, lambda turn: piece_copy(far, group, y_at(turn), y_me).start())

        loop(wide, one_group)

    def parts_stage(far):
        def wait_pieces(group):
            loop(tall - 1, lambda turn: piece_copy(far, group, y_at(turn), y_at(turn)).wait_recv())

        loop(wide, wait_pieces)

        @pl.when(far == 0)
        def _():
            for index in range(2):
                loop(wide - 1, lambda turn: weight_copy(index, x_at(turn), x_at(turn)).wait_recv())
                own_weight(index).wait()

        rows_of = jnp.concatenate(
            [
                jnp.concatenate([pieces[y, rows_at(group, far), :] for group in range(wide)], axis=0)
                for y in range(tall)
            ],
            axis=1,
        )
        parts = []
        for e in range(experts):
            block = jnp.concatenate(
                [weights[g, e].reshape(wide * own_hidden, features) for g in range(2)], axis=0
            )
            parts.append(dot_nt(rows_of, block))
        chosen_parts = choose(parts).astype(jnp.bfloat16)
        for group in range(wide):
            part_out[rows_at(group, far), :] = chosen_parts[
                group * half_rows : (group + 1) * half_rows
            ]
        loop(wide - 1, lambda turn: part_copy(far, x_at(turn), x_me).start())

        @pl.when(far == 0)
        def _():
            for index in range(early_weights, weight_count):
                send_weight(index)

    def hidden_stage(far):
        loop(wide - 1, lambda turn: part_copy(far, x_at(turn), x_at(turn)).wait_recv())
        total = part_out[rows_at(x_me, far), :].astype(jnp.float32)
        for turn in range(wide - 1):
            total = total + part_in[x_at(turn), far].astype(jnp.float32)
        middle = wide * own_hidden
        hidden = silu(total[:, 0:middle]) * total[:, middle:]
        hidden_all[y_me, far] = hidden.astype(jnp.bfloat16)
        loop(tall - 1, lambda turn: hidden_copy(far, y_at(turn), y_me).start())

    def down_stage(far):
        loop(tall - 1, lambda turn: hidden_copy(far, y_at(turn), y_at(turn)).wait_recv())

        @pl.when(far == 0)
        def _():
            for index in range(2, weight_count):
                loop(wide - 1, lambda turn: weight_copy(index, x_at(turn), x_at(turn)).wait_recv())
                own_weight(index).wait()

        units = jnp.concatenate([hidden_all[y, far] for y in range(tall)], axis=1)
        for x in range(0, wide, 2):
            results = [
                dot(units, jnp.concatenate([down_all[x, e], down_all[x + 1, e]], axis=1))
                for e in range(experts)
            ]
            result = choose(results).astype(jnp.bfloat16)
            columns = result.shape[1] // 2
            result_out[x, far] = result[:, 0:columns]
            result_out[x + 1, far] = result[:, columns:]
        loop(wide - 1, lambda turn: cross_copy(far, x_at(turn), x_me).start())
        own_cross(far).start()

    def return_stage(far):
        loop(wide - 1, lambda turn: cross_copy(far, x_at(turn), x_at(turn)).wait_recv())
        own_cross(far).wait()

        def one(rank):
            target = block_at(rank, far)

            @pl.when(target != me)
            def _():
                result_copy(target, me).start()

        loop(ep_count // 2, one)

        @pl.when(far == 0)
        def _():
            own_result().start()

    def received(hop, downward):
        going_up = jnp.logical_and(hop >= 1, jnp.logical_and(hop <= up_hops, chip - hop >= 0))
        source = lax.rem(chip + hop, chips)
        going_down = jnp.logical_and(
            hop >= 1, jnp.logical_and(hop <= down_hops, source <= last_down)
        )
        return jnp.where(downward, going_down, going_up)

    def useful(hop, downward):
        return jnp.logical_and(
            received(hop, downward), jnp.where(downward, chip + hop >= chips, True)
        )

    def forwards_up(hop):
        return jnp.logical_and(
            received(hop, False), jnp.logical_and(hop < up_hops, chip < chips - 1)
        )

    def forwards_down(hop):
        return jnp.logical_and(received(hop, True), hop < down_hops)

    def home_of(hop, downward):
        return jnp.where(downward, lax.rem(chip + hop, chips), chip - hop)

    def carry_on(part, hop, downward):
        slot = home_of(hop, downward) * CORES + core

        @pl.when(received(hop, downward))
        def _():
            up_copy(part, slot).wait_recv()

        if downward:

            @pl.when(forwards_down(hop))
            def _():
                down_copy(part, slot).start()

        else:

            @pl.when(forwards_up(hop))
            def _():
                up_copy(part, slot).start()

        @pl.when(useful(hop, downward))
        def _():
            side_copy(part, slot).start()

    def substep(index):
        @pl.when(jnp.logical_and(index >= 3, index % 3 == 0))
        def _():
            carry_on(0, index // 3, False)

        @pl.when(jnp.logical_and(index >= 3, index % 3 == 1))
        def _():
            carry_on(1, index // 3, False)
            carry_on(0, index // 3, True)

        @pl.when(jnp.logical_and(index >= 3, index % 3 == 2))
        def _():
            carry_on(1, index // 3, True)

        hop = index // 4
        kind = index % 4
        downward = kind % 2 == 1
        own_core = kind < 2
        slot = home_of(hop, downward) * CORES + jnp.where(own_core, core, other)
        sibling = jnp.logical_and(index == 2, core == 1)
        used = useful(hop, downward)

        @pl.when(jnp.logical_or(jnp.logical_and(jnp.logical_not(own_core), used), sibling))
        def _():
            for part in range(2):
                side_copy(part, slot).wait_recv()

        @pl.when(jnp.logical_or(used, sibling))
        def _():
            block_step(slot, held.at[slot], False)

        pl.when(index == LOCAL_AT)(local_stage)
        for stage, times in (
            (gather_stage, GATHER_AT),
            (parts_stage, PARTS_AT),
            (hidden_stage, HIDDEN_AT),
            (down_stage, DOWN_AT),
            (return_stage, RETURN_AT),
        ):
            far = jnp.where(index == times[1], 1, 0)

            @pl.when(jnp.logical_or(index == times[0], index == times[1]))
            def _():
                stage(far)

    loop(max(4 * up_hops + 4, RETURN_AT[1] + 1), substep, 2)

    heads = acc[0:HEAD] / acc[HEAD : HEAD + 1]
    heads_all[y_me, x_me] = heads.astype(jnp.bfloat16)
    loop(wide - 1, lambda turn: row_first(x_at(turn), x_me).start())
    loop(tall - 1, lambda turn: column_first(y_at(turn), y_me).start())
    loop(tall - 1, lambda turn: row_part(x_me, y_at(turn)).start())
    loop(wide - 1, lambda turn: column_part(y_me, x_at(turn)).start())

    def pass_row(turn):
        row_first(x_at(turn), x_at(turn)).wait_recv()
        loop(tall - 1, lambda way: row_part(x_at(turn), y_at(way)).start())

    def pass_column(turn):
        column_first(y_at(turn), y_at(turn)).wait_recv()
        loop(wide - 1, lambda way: column_part(y_at(turn), x_at(way)).start())

    loop(wide - 1, pass_row)
    loop(tall - 1, pass_column)

    loop(ep_count - 1, lambda turn: result_copy(ep_at(turn), ep_at(turn)).wait_recv())
    own_result().wait()
    loop(tp_count - 1, lambda turn: shared_copy(tp_at(turn), tp_at(turn)).wait_recv())
    shared_units = shared_all[...].reshape(tp_count * own_hidden, -1)
    shared_sum = dot(shared_weight[...], shared_units).T[0:tokens]
    routed = dot(spread[0], result_in[...]) + dot(spread[1], result_in[...])
    moe_ref[...] = (routed + shared_sum).astype(moe_ref.dtype)

    def finish_ep(turn):
        pick_copy(ep_at(turn), me).wait_send()
        result_copy(ep_at(turn), me).wait_send()

    loop(ep_count - 1, finish_ep)

    def finish_half(far):
        def finish_pieces(group):
            loop(tall - 1, lambda turn: piece_copy(far, group, y_at(turn), y_me).wait_send())

        loop(wide, finish_pieces)

        def finish_x(turn):
            part_copy(far, x_at(turn), x_me).wait_send()
            cross_copy(far, x_at(turn), x_me).wait_send()

        loop(wide - 1, finish_x)
        loop(tall - 1, lambda turn: hidden_copy(far, y_at(turn), y_me).wait_send())

    loop(2, finish_half)
    for index in range(weight_count):
        loop(wide - 1, lambda turn: weight_copy(index, x_at(turn), x_me).wait_send())
    loop(tp_count - 1, lambda turn: shared_copy(tp_at(turn), tp_me).wait_send())

    @pl.when(chip < chips - 1)
    def _():
        for part in range(2):
            up_copy(part, me, True).wait_send()

    @pl.when(chip <= last_down)
    def _():
        for part in range(2):
            down_copy(part, me, True).wait_send()

    @pl.when(core == 0)
    def _():
        for part in range(2):
            side_copy(part, me, True).wait_send()

    def finish_hop(hop):
        low_slot = home_of(hop, False) * CORES + core
        high_slot = home_of(hop, True) * CORES + core

        for part in range(2):

            @pl.when(forwards_up(hop))
            def _():
                up_copy(part, low_slot).wait_send()

            @pl.when(forwards_down(hop))
            def _():
                down_copy(part, high_slot).wait_send()

            @pl.when(useful(hop, False))
            def _():
                side_copy(part, low_slot).wait_send()

            @pl.when(useful(hop, True))
            def _():
                side_copy(part, high_slot).wait_send()

    loop(up_hops + 1, finish_hop, 1)

    def wait_far(turn):
        y = y_at(turn)

        def one(way):
            x = lax.rem(x_me + way, wide)
            column_copy(y, x, 0, 0, column_send.at[0, 0, 0]).wait_recv()

        loop(wide, one)

    def wait_wide(turn):
        x = x_at(turn)

        def one(way):
            y = lax.rem(y_me + way, tall)
            row_copy(y, x, 1, 0, row_send.at[0, 0, 0]).wait_recv()

        loop(tall, one)

    loop(tall - 1, wait_far)
    loop(wide - 1, wait_wide)
    for start in range(0, rows, tile):
        span = slice(start, start + tile)
        units = heads_all[:, :, :, span].reshape(tp_count * HEAD, tile)
        mixed = dot(mix_weight[...], units)
        mixer_ref[span, :] = mixed.T.astype(mixer_ref.dtype)

    def finish_row(turn):
        row_first(x_at(turn), x_me).wait_send()
        loop(tall, lambda y: column_part(y, x_at(turn)).wait_send())

    def finish_column(turn):
        column_first(y_at(turn), y_me).wait_send()
        loop(wide, lambda x: row_part(x, y_at(turn)).wait_send())

    loop(wide - 1, finish_row)
    loop(tall - 1, finish_column)


def slot_tables(ep_count, experts, cap, room):
    slot = np.arange(ep_count * room)
    inside = slot % room
    real = inside < experts * cap
    places = np.zeros((slot.size, 2 * LANES), np.float32)
    expert = (slot // room) * experts + inside // cap
    places[slot[real], expert[real]] = 1.0
    places[:, LANES] = np.where(real, -(inside % cap), 5.0)
    owner = np.where(real, inside // cap, 0).astype(np.float32)
    owner = np.tile(owner[: slot.size // 2, None], (1, LANES))
    return jnp.asarray(places, jnp.bfloat16), jnp.asarray(owner, jnp.float32)


def local(
    query_rows,
    key_rows,
    value_rows,
    cum_gate,
    out_weight,
    moe_input,
    moe_gain,
    routes,
    route_weight,
    expert_gate,
    expert_up,
    expert_down,
    shared_gate,
    shared_up,
    shared_down,
):
    rows, width = query_rows.shape
    token_count = moe_input.shape[0]
    top_count = routes.shape[1]
    experts, model, own_hidden = expert_gate.shape
    ep_count = lax.axis_size("ep")
    tp_count = lax.axis_size("tp")
    wide, tall = plane_shape(tp_count)
    expert_count = experts * ep_count
    cap = 2 * token_count * top_count // expert_count
    room = -(-experts * cap // 8) * 8
    slot_count = ep_count * room
    share_rows = slot_count // wide
    token_span = -(-token_count // LANES) * LANES
    columns = expert_down.shape[2]

    places, owner = slot_tables(ep_count, experts, cap, room)
    dma = pltpu.SemaphoreType.DMA
    vmem = pl.BlockSpec(memory_space=pltpu.VMEM)
    anywhere = pl.BlockSpec(memory_space=pl.ANY)
    blocks = ep_count * rows * rows
    bf16 = jnp.bfloat16
    mixer_out, moe_out = pl.pallas_call(
        functools.partial(layer_kernel, cap, room),
        out_shape=[
            jax.ShapeDtypeStruct((rows, columns), bf16),
            jax.ShapeDtypeStruct((token_count, columns), bf16),
        ],
        in_specs=[vmem] * 10 + [anywhere] * 3 + [vmem] * 4,
        out_specs=[vmem, vmem],
        scratch_shapes=[
            pltpu.VMEM((HEAD, rows), bf16),
            pltpu.VMEM((rows, LANES), bf16),
            pltpu.VMEM((rows, LANES), bf16),
            pltpu.VMEM((token_count, model), bf16),
            pltpu.VMEM((LANES, token_count), jnp.float32),
            pltpu.VMEM((LANES, token_count), jnp.float32),
            pltpu.VMEM((columns, tp_count * HEAD), bf16),
            pltpu.VMEM((columns, tp_count * own_hidden), bf16),
            pltpu.VMEM((ep_count, rows, LANES), bf16),
            pltpu.VMEM((HEAD + 16, rows), jnp.float32),
            pltpu.VMEM((8, rows), jnp.float32),
            pltpu.VMEM((slot_count, LANES), bf16),
            pltpu.VMEM((tall, slot_count, LANES), bf16),
            pltpu.VMEM((2, experts, wide, own_hidden, model // wide), bf16),
            pltpu.VMEM((wide, experts, tp_count * own_hidden, columns), bf16),
            pltpu.VMEM((slot_count, 2 * wide * own_hidden), bf16),
            pltpu.VMEM((wide, 2, share_rows // 2, 2 * wide * own_hidden), bf16),
            pltpu.VMEM((tall, 2, share_rows // 2, wide * own_hidden), bf16),
            pltpu.VMEM((own_hidden, token_span), bf16),
            pltpu.VMEM((tp_count, own_hidden, token_span), bf16),
            pltpu.VMEM((wide, 2, share_rows // 2, columns), bf16),
            pltpu.VMEM((slot_count, columns), bf16),
            pltpu.VMEM((slot_count, columns), bf16),
            pltpu.VMEM((2, token_count, slot_count), bf16),
            pltpu.VMEM((tall, wide, HEAD, rows), bf16),
        ]
        + [dma((2, ep_count))] * 4
        + [dma((ep_count,))] * 4
        + [dma((2, wide))] * 2
        + [dma((tall, 2 * wide))] * 2
        + [dma((2 + experts, wide))] * 2
        + [dma((2, wide))] * 2
        + [dma((2, tall))] * 2
        + [dma((tp_count,))] * 2
        + [dma((2, tall + 1, wide)), dma((2, wide + 1, tall)), dma((2, tp_count))]
        + [dma((experts + 4,)), dma((2,))],
        compiler_params=pltpu.CompilerParams(
            collective_id=0, has_side_effects=True, vmem_limit_bytes=56 * 1024 * 1024
        ),
        cost_estimate=pl.CostEstimate(
            flops=blocks * 2 * 512, bytes_accessed=8 * 1024 * 1024, transcendentals=blocks
        ),
        name="layer",
    )(
        query_rows.T,
        key_rows.T,
        value_rows.T,
        cum_gate.reshape(-1, LANES),
        moe_input,
        moe_gain.reshape(1, -1),
        routes.T,
        route_weight.T,
        places,
        owner,
        expert_gate.transpose(0, 2, 1),
        expert_up.transpose(0, 2, 1),
        expert_down,
        shared_gate.T,
        shared_up.T,
        shared_down,
        out_weight,
    )
    return mixer_out, moe_out


def solution(mesh):
    placed = (
        P("ep", "tp"),
        P("ep", "tp"),
        P("ep", "tp"),
        P("tp", None),
        P(None, "tp"),
        P("ep", None),
        P(),
        P("ep", None),
        P("ep", None),
        P("ep", None, "tp"),
        P("ep", None, "tp"),
        P("ep", None, "tp"),
        P(None, "tp"),
        P(None, "tp"),
        P(None, "tp"),
    )
    return jax.shard_map(
        local, mesh=mesh, in_specs=placed, out_specs=(P("ep", "tp"), P("ep", "tp")), check_vma=False
    )
```

```python
import functools

import jax
import jax.numpy as jnp
import numpy as np
from jax import lax
from jax.experimental import pallas as pl
from jax.experimental.pallas import tpu as pltpu
from jax.sharding import PartitionSpec as P

HEAD = 64
LANES = 128
CORES = 2
TERMS = 4
LOG2E = 1.4426950408889634

neg_fill = -1e30
norm_eps = 1e-06

LOCAL_AT = 5
GATHER_AT = (7, 10)
PARTS_AT = (9, 16)
HIDDEN_AT = (12, 20)
DOWN_AT = (19, 24)
RETURN_AT = (23, 28)


def plane_shape(tp_count):
    wide = 1
    while wide * wide < tp_count:
        wide *= 2
    return wide, tp_count // wide


def dot(a, b):
    return jnp.dot(a, b, preferred_element_type=jnp.float32)


def dot_nt(a, b):
    return lax.dot_general(a, b, (((1,), (1,)), ((), ())), preferred_element_type=jnp.float32)


def silu(v):
    return v / (1.0 + jnp.exp(-v))


def loop(count, body, first=0):
    def step(index, carry):
        body(index)
        return carry

    lax.fori_loop(first, count, step, 0)


def layer_kernel(
    cap,
    room,
    query_ref,
    key_ref,
    value_ref,
    gate_ref,
    input_ref,
    gain_ref,
    routes_ref,
    weight_ref,
    places_ref,
    owner_ref,
    gate_w,
    up_w,
    down_w,
    shared_gate_ref,
    shared_up_ref,
    shared_down_ref,
    out_weight_ref,
    mixer_ref,
    moe_ref,
    q_ref,
    kv_ref,
    terms_ref,
    normed_ref,
    weight_rows,
    rank_rows,
    mix_weight,
    shared_weight,
    held,
    acc,
    row_max,
    picked,
    pieces,
    weights,
    down_all,
    part_out,
    part_in,
    hidden_all,
    shared_out,
    shared_all,
    result_out,
    result_all,
    result_in,
    spread,
    heads_all,
    up_send,
    down_send,
    side_send,
    kv_recv,
    pick_send,
    pick_recv,
    result_send,
    result_recv,
    cross_send,
    cross_recv,
    piece_send,
    piece_recv,
    weight_send,
    weight_recv,
    part_send,
    part_recv,
    hidden_send,
    hidden_recv,
    shared_send,
    shared_recv,
    row_send,
    column_send,
    head_recv,
    own_sem,
    own_cross_sem,
):
    rows = q_ref.shape[1]
    half = rows // 2
    chunks = rows // LANES
    tile = 256 if rows % 256 == 0 else rows
    tokens = normed_ref.shape[0]
    experts = gate_w.shape[0]
    own_hidden = gate_w.shape[1]
    slot_count = picked.shape[0]
    slot_tile = 256 if slot_count % 256 == 0 else slot_count

    me = lax.axis_index("ep")
    ep_count = lax.axis_size("ep")
    chips = ep_count // CORES
    chip = me // CORES
    core = me % CORES
    other = 1 - core
    tp_count = lax.axis_size("tp")
    tp_me = lax.axis_index("tp")
    wide, tall = plane_shape(tp_count)
    x_me = tp_me % wide
    y_me = tp_me // wide
    up_hops = chips // 2
    down_hops = chips - 1 - up_hops
    last_down = chips - 2 - up_hops
    features = normed_ref.shape[1] // wide
    share = ep_count // wide
    share_rows = share * room
    half_share = share // 2
    half_rows = half_share * room
    reach = chips // 4

    def place_of(block, home):
        offset = lax.rem(block // CORES - home // CORES + reach + chips, chips)
        rank = lax.rem(offset, chips // 2) * CORES + block % CORES
        far = offset // (chips // 2)
        return rank // half_share * share + far * half_share + lax.rem(rank, half_share)

    def block_at(rank, far):
        offset = rank // CORES + far * (chips // 2)
        return lax.rem(chip - reach + offset + chips, chips) * CORES + rank % CORES

    def target_at(rank, far):
        offset = rank // CORES + far * (chips // 2)
        return lax.rem(chip + reach - offset + chips, chips) * CORES + rank % CORES

    def ep_at(turn):
        return lax.rem(me + turn + 1, ep_count)

    def tp_at(turn):
        return lax.rem(tp_me + turn + 1, tp_count)

    def x_at(turn):
        return lax.rem(x_me + turn + 1, wide)

    def y_at(turn):
        return lax.rem(y_me + turn + 1, tall)

    barrier = pltpu.get_barrier_semaphore()

    def greet(**where):
        pl.semaphore_signal(barrier, inc=1, device_id=where)

    loop(ep_count - 1, lambda turn: greet(ep=ep_at(turn)))
    loop(tp_count - 1, lambda turn: greet(tp=tp_at(turn)))

    def room_of(index):
        return pl.ds(pl.multiple_of(index * room, 8), room)

    def feature_lanes(index):
        return pl.ds(pl.multiple_of(index * features, LANES), features)

    model_rows = input_ref[...].astype(jnp.float32)
    scale = lax.rsqrt(jnp.mean(model_rows * model_rows, axis=1, keepdims=True) + norm_eps)
    normed_ref[...] = (model_rows * scale * gain_ref[...]).astype(jnp.bfloat16)

    expert_id = lax.broadcasted_iota(jnp.int32, (LANES, tokens), 0)
    named = jnp.zeros((LANES, tokens), jnp.float32)
    weight_of = jnp.zeros((LANES, tokens), jnp.float32)
    for j in range(routes_ref.shape[0]):
        match = routes_ref[j : j + 1, :] == expert_id
        named = jnp.where(match, 1.0, named)
        weight_of = jnp.where(match, weight_ref[j : j + 1, :], weight_of)
    before = lax.broadcasted_iota(jnp.int32, (tokens, tokens), 0)
    after = lax.broadcasted_iota(jnp.int32, (tokens, tokens), 1)
    earlier = jnp.where(before < after, 1.0, 0.0).astype(jnp.bfloat16)
    ranks = jnp.where(named > 0.0, dot(named.astype(jnp.bfloat16), earlier), -1.0)
    rank_rows[...] = ranks
    weight_rows[...] = weight_of

    piece_lanes = pl.ds(pl.multiple_of(x_me * features + y_me * LANES, LANES), LANES)
    line = lax.broadcasted_iota(jnp.int32, (LANES, tokens), 0)
    marker = jnp.where(line == 0, 1.0, 0.0).astype(jnp.bfloat16)
    marked = jnp.concatenate([ranks.astype(jnp.bfloat16), marker], axis=0)
    own_piece = normed_ref[:, piece_lanes]
    for start in range(0, slot_count, slot_tile):
        span = slice(start, start + slot_tile)
        match = dot(places_ref[span, :], marked)
        pick = jnp.where(match == 0.0, 1.0, 0.0).astype(jnp.bfloat16)
        picked[span, :] = dot(pick, own_piece).astype(jnp.bfloat16)

    q_ref[...] = (query_ref[...].astype(jnp.float32) * HEAD**-0.5).astype(jnp.bfloat16)
    lines = jnp.concatenate([key_ref[:, 0:half], key_ref[:, half:rows]], axis=0)
    kv_ref[0:half, :] = lines.astype(jnp.float32).T.astype(jnp.bfloat16)
    for i in range(chunks):
        kv_ref[half + HEAD * i : half + HEAD * (i + 1), :] = value_ref[:, LANES * i : LANES * (i + 1)]

    minus = -gate_ref[...].T
    high = minus.astype(jnp.bfloat16)
    rest = minus - high.astype(jnp.float32)
    middle = rest.astype(jnp.bfloat16)
    low = (rest - middle.astype(jnp.float32)).astype(jnp.bfloat16)
    gate_rows = gate_ref.shape[0]
    lane = lax.broadcasted_iota(jnp.int32, (gate_rows, LANES), 1)
    shift = lax.broadcasted_iota(jnp.int32, (gate_rows, LANES), 0) - (lane // TERMS) * chunks
    for i in range(chunks):
        terms = jnp.zeros((LANES, LANES), jnp.float32)
        for index, part in enumerate((high, middle, low)):
            spot = jnp.logical_and(shift == i, lane % TERMS == index)
            terms = terms + dot(part, jnp.where(spot, 1.0, 0.0).astype(jnp.bfloat16))
        terms_ref[LANES * i : LANES * (i + 1), :] = terms.astype(jnp.bfloat16)

    acc[...] = jnp.zeros_like(acc)
    row_max[...] = jnp.full_like(row_max, neg_fill)

    pl.semaphore_wait(barrier, ep_count + tp_count - 2)

    def pick_copy(target, owner):
        return pltpu.make_async_remote_copy(
            src_ref=picked.at[room_of(target)],
            dst_ref=pieces.at[y_me, room_of(place_of(owner, target))],
            send_sem=pick_send.at[target],
            recv_sem=pick_recv.at[owner],
            device_id={"ep": target},
        )

    def weight_ends(index, target, owner):
        if index < 2:
            source = (gate_w, up_w)[index].at[:, :, feature_lanes(target)]
            return source, weights.at[index, :, owner]
        return down_w.at[index - 2], down_all.at[owner, index - 2]

    def weight_copy(index, target, owner):
        source, place = weight_ends(index, target, owner)
        return pltpu.make_async_remote_copy(
            src_ref=source,
            dst_ref=place,
            send_sem=weight_send.at[index, target],
            recv_sem=weight_recv.at[index, owner],
            device_id={"tp": y_me * wide + target},
        )

    def own_weight(index):
        source, place = weight_ends(index, x_me, x_me)
        return pltpu.make_async_copy(source, place, own_sem.at[index])

    weight_count = 2 + experts
    early_weights = 2 + experts // 2

    def send_weight(index):
        loop(wide - 1, lambda turn: weight_copy(index, x_at(turn), x_me).start())

    def kv_copy(part, slot, own, send_sem, place):
        span = pl.ds(part * half, half)
        return pltpu.make_async_remote_copy(
            src_ref=kv_ref.at[span] if own else held.at[slot, span],
            dst_ref=held.at[slot, span],
            send_sem=send_sem.at[part, slot],
            recv_sem=kv_recv.at[part, slot],
            device_id={"ep": place},
        )

    def up_copy(part, slot, own=False):
        return kv_copy(part, slot, own, up_send, me + CORES)

    def down_copy(part, slot, own=False):
        below = lax.rem(chip + chips - 1, chips) * CORES + core
        return kv_copy(part, slot, own, down_send, below)

    def side_copy(part, slot, own=False):
        return kv_copy(part, slot, own, side_send, chip * CORES + other)

    def piece_copy(far, group, target, owner):
        place = pieces.at[owner, rows_at(group, far)]
        return pltpu.make_async_remote_copy(
            src_ref=place,
            dst_ref=place,
            send_sem=piece_send.at[target, far * wide + group],
            recv_sem=piece_recv.at[owner, far * wide + group],
            device_id={"tp": target * wide + x_me},
        )

    def part_copy(far, target, owner):
        return pltpu.make_async_remote_copy(
            src_ref=part_out.at[rows_at(target, far)],
            dst_ref=part_in.at[owner, far],
            send_sem=part_send.at[far, target],
            recv_sem=part_recv.at[far, owner],
            device_id={"tp": y_me * wide + target},
        )

    def hidden_copy(far, target, owner):
        return pltpu.make_async_remote_copy(
            src_ref=hidden_all.at[owner, far],
            dst_ref=hidden_all.at[owner, far],
            send_sem=hidden_send.at[far, target],
            recv_sem=hidden_recv.at[far, owner],
            device_id={"tp": target * wide + x_me},
        )

    def shared_copy(target, owner):
        return pltpu.make_async_remote_copy(
            src_ref=shared_out,
            dst_ref=shared_all.at[owner],
            send_sem=shared_send.at[target],
            recv_sem=shared_recv.at[owner],
            device_id={"tp": target},
        )

    def rows_at(index, far):
        start = index * share_rows + far * half_rows
        return pl.ds(pl.multiple_of(start, 8), half_rows)

    def cross_copy(far, target, owner):
        return pltpu.make_async_remote_copy(
            src_ref=result_out.at[target, far],
            dst_ref=result_all.at[rows_at(owner, far)],
            send_sem=cross_send.at[far, target],
            recv_sem=cross_recv.at[far, owner],
            device_id={"tp": y_me * wide + target},
        )

    def own_cross(far):
        return pltpu.make_async_copy(
            result_out.at[x_me, far], result_all.at[rows_at(x_me, far)], own_cross_sem.at[far]
        )

    def result_copy(target, owner):
        return pltpu.make_async_remote_copy(
            src_ref=result_all.at[room_of(place_of(target, me))],
            dst_ref=result_in.at[room_of(owner)],
            send_sem=result_send.at[target],
            recv_sem=result_recv.at[owner],
            device_id={"ep": target},
        )

    def own_result():
        return pltpu.make_async_copy(
            result_all.at[room_of(place_of(me, me))],
            result_in.at[room_of(me)],
            own_sem.at[weight_count],
        )

    half_head = HEAD // 2

    def row_copy(owner_y, owner_x, part, target, sem):
        place = heads_all.at[owner_y, owner_x, part * half_head : (part + 1) * half_head]
        return pltpu.make_async_remote_copy(
            src_ref=place,
            dst_ref=place,
            send_sem=sem,
            recv_sem=head_recv.at[part, owner_y * wide + owner_x],
            device_id={"tp": y_me * wide + target},
        )

    def column_copy(owner_y, owner_x, part, target, sem):
        place = heads_all.at[owner_y, owner_x, part * half_head : (part + 1) * half_head]
        return pltpu.make_async_remote_copy(
            src_ref=place,
            dst_ref=place,
            send_sem=sem,
            recv_sem=head_recv.at[part, owner_y * wide + owner_x],
            device_id={"tp": target * wide + x_me},
        )

    def row_part(owner_x, target):
        return column_copy(y_me, owner_x, 0, target, column_send.at[0, owner_x, target])

    def row_first(target, owner_x):
        return row_copy(y_me, owner_x, 0, target, row_send.at[1, tall, target])

    def column_part(owner_y, target):
        return row_copy(owner_y, x_me, 1, target, row_send.at[0, owner_y, target])

    def column_first(target, owner_y):
        return column_copy(owner_y, x_me, 1, target, column_send.at[1, wide, target])

    def own_pick():
        return pltpu.make_async_copy(
            picked.at[room_of(me)],
            pieces.at[y_me, room_of(place_of(me, me))],
            own_sem.at[weight_count + 1],
        )

    @pl.when(chip < chips - 1)
    def _():
        for part in range(2):
            up_copy(part, me, True).start()

    @pl.when(chip <= last_down)
    def _():
        for part in range(2):
            down_copy(part, me, True).start()

    @pl.when(core == 0)
    def _():
        for part in range(2):
            side_copy(part, me, True).start()

    def send_picked(far):
        def one(rank):
            target = target_at(rank, far)

            @pl.when(target != me)
            def _():
                pick_copy(target, me).start()

        loop(ep_count // 2, one)

    send_picked(0)
    own_pick().start()
    for index in range(weight_count):
        own_weight(index).start()
    for index in range(early_weights):
        send_weight(index)

    ones = jnp.ones((acc.shape[0] - HEAD, rows), jnp.bfloat16)
    nothing = jnp.zeros((HEAD, tile), jnp.bfloat16)

    def block_step(block, source, masked):
        mark = lax.broadcasted_iota(jnp.int32, (LANES, tile), 0)
        wanted = jnp.logical_and(mark // TERMS == block, mark % TERMS < TERMS - 1)
        chosen = jnp.where(wanted, 1.0, 0.0).astype(jnp.bfloat16)
        keys = source[0:half, :]
        early = jnp.concatenate([keys, terms_ref[0:half, :]], axis=1)
        late = jnp.concatenate([keys, terms_ref[half:rows, :]], axis=1)
        values = jnp.concatenate(
            [source[half + HEAD * i : half + HEAD * (i + 1), :] for i in range(chunks)], axis=1
        )
        values = jnp.concatenate([values, ones], axis=0)

        def score(start):
            query = q_ref[:, start : start + tile]
            first = dot(early, jnp.concatenate([query, nothing, chosen], axis=0))
            second = dot(late, jnp.concatenate([nothing, query, chosen], axis=0))
            if masked:
                q_pos = start + lax.broadcasted_iota(jnp.int32, first.shape, 1)
                k_pos = lax.broadcasted_iota(jnp.int32, first.shape, 0)
                first = jnp.where(k_pos <= q_pos, first, neg_fill)
                second = jnp.where(k_pos + half <= q_pos, second, neg_fill)
            return first, second

        def soften(start, first, second):
            old_max = row_max[0:1, start : start + tile]
            top = jnp.maximum(
                jnp.max(first, axis=0, keepdims=True), jnp.max(second, axis=0, keepdims=True)
            )
            new_max = jnp.maximum(old_max, top)
            probs = jnp.concatenate(
                [
                    jnp.exp2((first - new_max) * LOG2E).astype(jnp.bfloat16),
                    jnp.exp2((second - new_max) * LOG2E).astype(jnp.bfloat16),
                ],
                axis=0,
            )
            row_max[0:1, start : start + tile] = new_max
            return probs, jnp.exp2((old_max - new_max) * LOG2E)

        def collect(start, probs, keep):
            span = slice(start, start + tile)
            acc[:, span] = acc[:, span] * keep + dot(values, probs)

        starts = list(range(0, rows, tile))
        scores = score(starts[0])
        waiting = None
        for index, start in enumerate(starts):
            upcoming = score(starts[index + 1]) if index + 1 < len(starts) else None
            ready = soften(start, *scores)
            if waiting is not None:
                collect(starts[index - 1], *waiting)
            waiting, scores = ready, upcoming
        collect(starts[-1], *waiting)

    block_step(me, kv_ref, True)

    def local_stage():
        send_picked(1)

        column = lax.broadcasted_iota(jnp.int32, (tokens, LANES), 1)
        marker = jnp.where(column == 0, 1.0, 0.0).astype(jnp.bfloat16)
        marked = jnp.concatenate([rank_rows[...].T.astype(jnp.bfloat16), marker], axis=1)
        weight = weight_rows[...].T
        high = weight.astype(jnp.bfloat16)
        low = (weight - high.astype(jnp.float32)).astype(jnp.bfloat16)
        for start in range(0, slot_count, slot_tile):
            span = slice(start, start + slot_tile)
            match = dot_nt(marked, places_ref[span, :])
            for index, part in enumerate((high, low)):
                value = dot_nt(part, places_ref[span, 0:LANES])
                spread[index, :, span] = jnp.where(match == 0.0, value, 0.0).astype(jnp.bfloat16)
        shared = silu(dot_nt(shared_gate_ref[...], normed_ref[...])) * dot_nt(
            shared_up_ref[...], normed_ref[...]
        )
        shared_out[...] = jnp.zeros_like(shared_out)
        shared_out[:, 0:tokens] = shared.astype(jnp.bfloat16)
        shared_all[tp_me] = shared_out[...]
        loop(tp_count - 1, lambda turn: shared_copy(tp_at(turn), tp_me).start())
        mix_weight[...] = out_weight_ref[...].astype(jnp.float32).T.astype(jnp.bfloat16)
        shared_weight[...] = shared_down_ref[...].astype(jnp.float32).T.astype(jnp.bfloat16)

    def choose(parts):
        owner = owner_ref[0 : parts[0].shape[0], 0:1]
        value = parts[0]
        for index in range(1, experts):
            value = jnp.where(owner == float(index), parts[index], value)
        return value

    def gather_stage(far):
        @pl.when(far == 0)
        def _():
            own_pick().wait()

        def one_group(group):
            def wait_block(turn):
                source = block_at(group * half_share + turn, far)

                @pl.when(source != me)
                def _():
                    pick_copy(source, source).wait_recv()

            loop(half_share, wait_block)
            loop(tall - 1, lambda turn: piece_copy(far, group, y_at(turn), y_me).start())

        loop(wide, one_group)

    def parts_stage(far):
        def wait_pieces(group):
            loop(tall - 1, lambda turn: piece_copy(far, group, y_at(turn), y_at(turn)).wait_recv())

        loop(wide, wait_pieces)

        @pl.when(far == 0)
        def _():
            for index in range(2):
                loop(wide - 1, lambda turn: weight_copy(index, x_at(turn), x_at(turn)).wait_recv())
                own_weight(index).wait()

        rows_of = jnp.concatenate(
            [
                jnp.concatenate([pieces[y, rows_at(group, far), :] for group in range(wide)], axis=0)
                for y in range(tall)
            ],
            axis=1,
        )
        parts = []
        for e in range(experts):
            block = jnp.concatenate(
                [weights[g, e].reshape(wide * own_hidden, features) for g in range(2)], axis=0
            )
            parts.append(dot_nt(rows_of, block))
        chosen_parts = choose(parts).astype(jnp.bfloat16)
        for group in range(wide):
            part_out[rows_at(group, far), :] = chosen_parts[
                group * half_rows : (group + 1) * half_rows
            ]
        loop(wide - 1, lambda turn: part_copy(far, x_at(turn), x_me).start())

        @pl.when(far == 0)
        def _():
            for index in range(early_weights, weight_count):
                send_weight(index)

    def hidden_stage(far):
        loop(wide - 1, lambda turn: part_copy(far, x_at(turn), x_at(turn)).wait_recv())
        total = part_out[rows_at(x_me, far), :].astype(jnp.float32)
        for turn in range(wide - 1):
            total = total + part_in[x_at(turn), far].astype(jnp.float32)
        middle = wide * own_hidden
        hidden = silu(total[:, 0:middle]) * total[:, middle:]
        hidden_all[y_me, far] = hidden.astype(jnp.bfloat16)
        loop(tall - 1, lambda turn: hidden_copy(far, y_at(turn), y_me).start())

    def down_stage(far):
        loop(tall - 1, lambda turn: hidden_copy(far, y_at(turn), y_at(turn)).wait_recv())

        @pl.when(far == 0)
        def _():
            for index in range(2, weight_count):
                loop(wide - 1, lambda turn: weight_copy(index, x_at(turn), x_at(turn)).wait_recv())
                own_weight(index).wait()

        units = jnp.concatenate([hidden_all[y, far] for y in range(tall)], axis=1)
        for x in range(0, wide, 2):
            results = [
                dot(units, jnp.concatenate([down_all[x, e], down_all[x + 1, e]], axis=1))
                for e in range(experts)
            ]
            result = choose(results).astype(jnp.bfloat16)
            columns = result.shape[1] // 2
            result_out[x, far] = result[:, 0:columns]
            result_out[x + 1, far] = result[:, columns:]
        loop(wide - 1, lambda turn: cross_copy(far, x_at(turn), x_me).start())
        own_cross(far).start()

    def return_stage(far):
        loop(wide - 1, lambda turn: cross_copy(far, x_at(turn), x_at(turn)).wait_recv())
        own_cross(far).wait()

        def one(rank):
            target = block_at(rank, far)

            @pl.when(target != me)
            def _():
                result_copy(target, me).start()

        loop(ep_count // 2, one)

        @pl.when(far == 0)
        def _():
            own_result().start()

    def received(hop, downward):
        going_up = jnp.logical_and(hop >= 1, jnp.logical_and(hop <= up_hops, chip - hop >= 0))
        source = lax.rem(chip + hop, chips)
        going_down = jnp.logical_and(
            hop >= 1, jnp.logical_and(hop <= down_hops, source <= last_down)
        )
        return jnp.where(downward, going_down, going_up)

    def useful(hop, downward):
        return jnp.logical_and(
            received(hop, downward), jnp.where(downward, chip + hop >= chips, True)
        )

    def forwards_up(hop):
        return jnp.logical_and(
            received(hop, False), jnp.logical_and(hop < up_hops, chip < chips - 1)
        )

    def forwards_down(hop):
        return jnp.logical_and(received(hop, True), hop < down_hops)

    def home_of(hop, downward):
        return jnp.where(downward, lax.rem(chip + hop, chips), chip - hop)

    def carry_on(part, hop, downward):
        slot = home_of(hop, downward) * CORES + core

        @pl.when(received(hop, downward))
        def _():
            up_copy(part, slot).wait_recv()

        if downward:

            @pl.when(forwards_down(hop))
            def _():
                down_copy(part, slot).start()

        else:

            @pl.when(forwards_up(hop))
            def _():
                up_copy(part, slot).start()

        @pl.when(useful(hop, downward))
        def _():
            side_copy(part, slot).start()

    def substep(index):
        @pl.when(jnp.logical_and(index >= 3, index % 3 == 0))
        def _():
            carry_on(0, index // 3, False)

        @pl.when(jnp.logical_and(index >= 3, index % 3 == 1))
        def _():
            carry_on(1, index // 3, False)
            carry_on(0, index // 3, True)

        @pl.when(jnp.logical_and(index >= 3, index % 3 == 2))
        def _():
            carry_on(1, index // 3, True)

        hop = index // 4
        kind = index % 4
        downward = kind % 2 == 1
        own_core = kind < 2
        slot = home_of(hop, downward) * CORES + jnp.where(own_core, core, other)
        sibling = jnp.logical_and(index == 2, core == 1)
        used = useful(hop, downward)

        @pl.when(jnp.logical_or(jnp.logical_and(jnp.logical_not(own_core), used), sibling))
        def _():
            for part in range(2):
                side_copy(part, slot).wait_recv()

        @pl.when(jnp.logical_or(used, sibling))
        def _():
            block_step(slot, held.at[slot], False)

        pl.when(index == LOCAL_AT)(local_stage)
        for stage, times in (
            (gather_stage, GATHER_AT),
            (parts_stage, PARTS_AT),
            (hidden_stage, HIDDEN_AT),
            (down_stage, DOWN_AT),
            (return_stage, RETURN_AT),
        ):
            far = jnp.where(index == times[1], 1, 0)

            @pl.when(jnp.logical_or(index == times[0], index == times[1]))
            def _():
                stage(far)

    loop(max(4 * up_hops + 4, RETURN_AT[1] + 1), substep, 2)

    heads = acc[0:HEAD] / acc[HEAD : HEAD + 1]
    heads_all[y_me, x_me] = heads.astype(jnp.bfloat16)
    loop(wide - 1, lambda turn: row_first(x_at(turn), x_me).start())
    loop(tall - 1, lambda turn: column_first(y_at(turn), y_me).start())
    loop(tall - 1, lambda turn: row_part(x_me, y_at(turn)).start())
    loop(wide - 1, lambda turn: column_part(y_me, x_at(turn)).start())

    def pass_row(turn):
        row_first(x_at(turn), x_at(turn)).wait_recv()
        loop(tall - 1, lambda way: row_part(x_at(turn), y_at(way)).start())

    def pass_column(turn):
        column_first(y_at(turn), y_at(turn)).wait_recv()
        loop(wide - 1, lambda way: column_part(y_at(turn), x_at(way)).start())

    def finish_ep(turn):
        pick_copy(ep_at(turn), me).wait_send()

    loop(ep_count - 1, finish_ep)

    def finish_half(far):
        def finish_pieces(group):
            loop(tall - 1, lambda turn: piece_copy(far, group, y_at(turn), y_me).wait_send())

        loop(wide, finish_pieces)

        def finish_x(turn):
            part_copy(far, x_at(turn), x_me).wait_send()
            cross_copy(far, x_at(turn), x_me).wait_send()

        loop(wide - 1, finish_x)
        loop(tall - 1, lambda turn: hidden_copy(far, y_at(turn), y_me).wait_send())

    loop(2, finish_half)
    for index in range(weight_count):
        loop(wide - 1, lambda turn: weight_copy(index, x_at(turn), x_me).wait_send())
    loop(tp_count - 1, lambda turn: shared_copy(tp_at(turn), tp_me).wait_send())

    @pl.when(chip < chips - 1)
    def _():
        for part in range(2):
            up_copy(part, me, True).wait_send()

    @pl.when(chip <= last_down)
    def _():
        for part in range(2):
            down_copy(part, me, True).wait_send()

    @pl.when(core == 0)
    def _():
        for part in range(2):
            side_copy(part, me, True).wait_send()

    def finish_hop(hop):
        low_slot = home_of(hop, False) * CORES + core
        high_slot = home_of(hop, True) * CORES + core

        for part in range(2):

            @pl.when(forwards_up(hop))
            def _():
                up_copy(part, low_slot).wait_send()

            @pl.when(forwards_down(hop))
            def _():
                down_copy(part, high_slot).wait_send()

            @pl.when(useful(hop, False))
            def _():
                side_copy(part, low_slot).wait_send()

            @pl.when(useful(hop, True))
            def _():
                side_copy(part, high_slot).wait_send()

    loop(up_hops + 1, finish_hop, 1)

    loop(wide - 1, pass_row)
    loop(tall - 1, pass_column)

    loop(tp_count - 1, lambda turn: shared_copy(tp_at(turn), tp_at(turn)).wait_recv())
    shared_units = shared_all[...].reshape(tp_count * own_hidden, -1)
    shared_sum = dot(shared_weight[...], shared_units).T[0:tokens]

    def wait_far(turn):
        y = y_at(turn)

        def one(way):
            x = lax.rem(x_me + way, wide)
            column_copy(y, x, 0, 0, column_send.at[0, 0, 0]).wait_recv()

        loop(wide, one)

    def wait_wide(turn):
        x = x_at(turn)

        def one(way):
            y = lax.rem(y_me + way, tall)
            row_copy(y, x, 1, 0, row_send.at[0, 0, 0]).wait_recv()

        loop(tall, one)

    loop(tall - 1, wait_far)
    loop(wide - 1, wait_wide)
    for start in range(0, rows, tile):
        span = slice(start, start + tile)
        units = heads_all[:, :, :, span].reshape(tp_count * HEAD, tile)
        mixed = dot(mix_weight[...], units)
        mixer_ref[span, :] = mixed.T.astype(mixer_ref.dtype)

    loop(ep_count - 1, lambda turn: result_copy(ep_at(turn), ep_at(turn)).wait_recv())
    own_result().wait()
    routed = dot(spread[0], result_in[...]) + dot(spread[1], result_in[...])
    moe_ref[...] = (routed + shared_sum).astype(moe_ref.dtype)

    def finish_row(turn):
        row_first(x_at(turn), x_me).wait_send()
        loop(tall, lambda y: column_part(y, x_at(turn)).wait_send())

    def finish_column(turn):
        column_first(y_at(turn), y_me).wait_send()
        loop(wide, lambda x: row_part(x, y_at(turn)).wait_send())

    loop(ep_count - 1, lambda turn: result_copy(ep_at(turn), me).wait_send())
    loop(wide - 1, finish_row)
    loop(tall - 1, finish_column)


def slot_tables(ep_count, experts, cap, room):
    slot = np.arange(ep_count * room)
    inside = slot % room
    real = inside < experts * cap
    places = np.zeros((slot.size, 2 * LANES), np.float32)
    expert = (slot // room) * experts + inside // cap
    places[slot[real], expert[real]] = 1.0
    places[:, LANES] = np.where(real, -(inside % cap), 5.0)
    owner = np.where(real, inside // cap, 0).astype(np.float32)
    owner = np.tile(owner[: slot.size // 2, None], (1, LANES))
    return jnp.asarray(places, jnp.bfloat16), jnp.asarray(owner, jnp.float32)


def local(
    query_rows,
    key_rows,
    value_rows,
    cum_gate,
    out_weight,
    moe_input,
    moe_gain,
    routes,
    route_weight,
    expert_gate,
    expert_up,
    expert_down,
    shared_gate,
    shared_up,
    shared_down,
):
    rows, width = query_rows.shape
    token_count = moe_input.shape[0]
    top_count = routes.shape[1]
    experts, model, own_hidden = expert_gate.shape
    ep_count = lax.axis_size("ep")
    tp_count = lax.axis_size("tp")
    wide, tall = plane_shape(tp_count)
    expert_count = experts * ep_count
    cap = 2 * token_count * top_count // expert_count
    room = -(-experts * cap // 8) * 8
    slot_count = ep_count * room
    share_rows = slot_count // wide
    token_span = -(-token_count // LANES) * LANES
    columns = expert_down.shape[2]

    places, owner = slot_tables(ep_count, experts, cap, room)
    dma = pltpu.SemaphoreType.DMA
    vmem = pl.BlockSpec(memory_space=pltpu.VMEM)
    anywhere = pl.BlockSpec(memory_space=pl.ANY)
    blocks = ep_count * rows * rows
    bf16 = jnp.bfloat16
    mixer_out, moe_out = pl.pallas_call(
        functools.partial(layer_kernel, cap, room),
        out_shape=[
            jax.ShapeDtypeStruct((rows, columns), bf16),
            jax.ShapeDtypeStruct((token_count, columns), bf16),
        ],
        in_specs=[vmem] * 10 + [anywhere] * 3 + [vmem] * 4,
        out_specs=[vmem, vmem],
        scratch_shapes=[
            pltpu.VMEM((HEAD, rows), bf16),
            pltpu.VMEM((rows, LANES), bf16),
            pltpu.VMEM((rows, LANES), bf16),
            pltpu.VMEM((token_count, model), bf16),
            pltpu.VMEM((LANES, token_count), jnp.float32),
            pltpu.VMEM((LANES, token_count), jnp.float32),
            pltpu.VMEM((columns, tp_count * HEAD), bf16),
            pltpu.VMEM((columns, tp_count * own_hidden), bf16),
            pltpu.VMEM((ep_count, rows, LANES), bf16),
            pltpu.VMEM((HEAD + 16, rows), jnp.float32),
            pltpu.VMEM((8, rows), jnp.float32),
            pltpu.VMEM((slot_count, LANES), bf16),
            pltpu.VMEM((tall, slot_count, LANES), bf16),
            pltpu.VMEM((2, experts, wide, own_hidden, model // wide), bf16),
            pltpu.VMEM((wide, experts, tp_count * own_hidden, columns), bf16),
            pltpu.VMEM((slot_count, 2 * wide * own_hidden), bf16),
            pltpu.VMEM((wide, 2, share_rows // 2, 2 * wide * own_hidden), bf16),
            pltpu.VMEM((tall, 2, share_rows // 2, wide * own_hidden), bf16),
            pltpu.VMEM((own_hidden, token_span), bf16),
            pltpu.VMEM((tp_count, own_hidden, token_span), bf16),
            pltpu.VMEM((wide, 2, share_rows // 2, columns), bf16),
            pltpu.VMEM((slot_count, columns), bf16),
            pltpu.VMEM((slot_count, columns), bf16),
            pltpu.VMEM((2, token_count, slot_count), bf16),
            pltpu.VMEM((tall, wide, HEAD, rows), bf16),
        ]
        + [dma((2, ep_count))] * 4
        + [dma((ep_count,))] * 4
        + [dma((2, wide))] * 2
        + [dma((tall, 2 * wide))] * 2
        + [dma((2 + experts, wide))] * 2
        + [dma((2, wide))] * 2
        + [dma((2, tall))] * 2
        + [dma((tp_count,))] * 2
        + [dma((2, tall + 1, wide)), dma((2, wide + 1, tall)), dma((2, tp_count))]
        + [dma((experts + 4,)), dma((2,))],
        compiler_params=pltpu.CompilerParams(
            collective_id=0, has_side_effects=True, vmem_limit_bytes=56 * 1024 * 1024
        ),
        cost_estimate=pl.CostEstimate(
            flops=blocks * 2 * 512, bytes_accessed=8 * 1024 * 1024, transcendentals=blocks
        ),
        name="layer",
    )(
        query_rows.T,
        key_rows.T,
        value_rows.T,
        cum_gate.reshape(-1, LANES),
        moe_input,
        moe_gain.reshape(1, -1),
        routes.T,
        route_weight.T,
        places,
        owner,
        expert_gate.transpose(0, 2, 1),
        expert_up.transpose(0, 2, 1),
        expert_down,
        shared_gate.T,
        shared_up.T,
        shared_down,
        out_weight,
    )
    return mixer_out, moe_out


def solution(mesh):
    placed = (
        P("ep", "tp"),
        P("ep", "tp"),
        P("ep", "tp"),
        P("tp", None),
        P(None, "tp"),
        P("ep", None),
        P(),
        P("ep", None),
        P("ep", None),
        P("ep", None, "tp"),
        P("ep", None, "tp"),
        P("ep", None, "tp"),
        P(None, "tp"),
        P(None, "tp"),
        P(None, "tp"),
    )
    return jax.shard_map(
        local, mesh=mesh, in_specs=placed, out_specs=(P("ep", "tp"), P("ep", "tp")), check_vma=False
    )
```
